256 devices in a mesh: sp: 64 (over z, x, core), tp: 4 (over y).
Axes of the slice: x: 4, y: 4, z: 8, core: 2. Of those that a mesh axis runs over, the one named last changes fastest.
Arguments:
- queries: bfloat16 [8192, 1024], P('sp', 'tp'), may hold values from -160 to 160
- keys: bfloat16 [8192, 256], P('sp', 'tp'), may hold values from -5 to 5
- values: bfloat16 [8192, 256], P('sp', 'tp'), may hold values from -6 to 6
- cum_gate: float32 [8192, 16], P('sp', 'tp'), as said below
- doc_ids: int32 [8192], P('sp'), may hold values from 0 to 7, never falling along the last dimension, each value on 1 to 4224 neighbouring positions
- residual: bfloat16 [8192, 2048], P(('sp', 'tp')), may hold values from -6 to 6
- out_proj: bfloat16 [1024, 2048], replicated, may hold values from -0.1875 to 0.1875
- norm_gain: float32 [2048], replicated, may hold values from 0.1 to 1.9
- route_ids: int32 [8192, 2], P(('sp', 'tp')), may hold values from 0 to 63, all different within a row; in each aligned block of 32 rows (0 to 31, 32 to 63, ...) at most 2 rows name the same one
- route_weights: float32 [8192, 2], P(('sp', 'tp')), may hold values from 0.2 to 1
- expert_gate: bfloat16 [64, 2048, 1024], P('sp', None, 'tp'), may hold values from -0.125 to 0.125
- expert_up: bfloat16 [64, 2048, 1024], P('sp', None, 'tp'), may hold values from -0.125 to 0.125
- expert_down: bfloat16 [64, 1024, 2048], P('sp', 'tp'), may hold values from -0.1875 to 0.1875
Outputs:
- mixed: bfloat16 [8192, 2048], P(('sp', 'tp'))
The draws below stay inside these ranges and needn't reach their ends.
Inputs may be any that keep to these rules, and one draw needn't show every extreme that they name: `route_ids`: within each aligned block of 32 rows no expert is named by more than 2 rows, and in every draw some block has an expert named by exactly 2 rows; the 2 experts of a row differ. `doc_ids`: never falling along positions; a document spans at most 4224 positions, and one spans exactly that many. `cum_gate`: never rising along positions.
All inputs are finite; a program needn't handle non-finite values.
Results may differ from the reference program's by a relative error of at most 0.014.
Values may be sent and summed in bfloat16 or wider, within the bound.
A program may use at most 128 MiB of HBM per device.

```python
import math
import jax
import jax.numpy as jnp
import numpy as np
from jax import lax

D = 2048
ASKING_PLANES = 16
HEAD_DIM = 64
KV_HEADS = 4
EXPERT_FF = 1024
TOP = 2
DOCS = 8
TOK_DEV = 128
TEXT_SLOTS = 8192
ROWS_DEV = 32
EXPERTS = 64
CAP = 2
DOC_MOST = 4224
N_TP = 4


def shared_keys(key):
    shared = jax.random.fold_in(key, 7)
    drawn = jax.random.normal(jax.random.fold_in(shared, 1), (TEXT_SLOTS, KV_HEADS * HEAD_DIM), jnp.float32)
    drawn = jnp.clip(drawn, -5.0, 5.0)
    return drawn


def draw_keys(key, part):
    drawn = shared_keys(key)
    return drawn.astype(jnp.bfloat16)


def draw_queries(key, part):
    entries = jax.random.normal(jax.random.fold_in(key, 31), (TEXT_SLOTS, ASKING_PLANES * HEAD_DIM), jnp.float32)
    entries = 3.0 * jnp.clip(entries, -6.0, 6.0)
    return entries.astype(jnp.bfloat16)


def draw_cum_gate(key, part):
    lane_number = jax.random.split(jax.random.fold_in(key, 11), 7)
    order = jax.random.permutation(lane_number[0], ASKING_PLANES)
    keeping = ASKING_PLANES // 2
    slow = order < keeping
    slow_total = jax.random.uniform(lane_number[1], (ASKING_PLANES,), jnp.float32, 0.2, 0.8)
    fast_rate = jnp.exp(jax.random.uniform(lane_number[2], (ASKING_PLANES,), jnp.float32, math.log(1.0 / 100.0), math.log(1.0 / 30.0)))
    rate = jnp.where(slow, slow_total / TEXT_SLOTS, fast_rate)
    block_scaling = jnp.exp(jax.random.uniform(lane_number[3], (TEXT_SLOTS // TOK_DEV,), jnp.float32, math.log(0.5), math.log(2.0)))
    block_of = jnp.arange(TEXT_SLOTS, dtype=jnp.int32) // TOK_DEV
    jitter = jax.random.uniform(lane_number[4], (TEXT_SLOTS, ASKING_PLANES), jnp.float32, 0.5, 1.5)
    iteration_total = -rate[None, :] * block_scaling[block_of][:, None] * jitter
    span_offset = jax.random.randint(lane_number[5], (3,), 0, TEXT_SLOTS)
    span_extent = jax.random.uniform(lane_number[6], (3, ASKING_PLANES), jnp.float32, 0.22, 0.69)
    iteration_total = iteration_total.at[span_offset].add(-span_extent)
    return jnp.cumsum(iteration_total, axis=0)


def shard_levels(rng, extent, shards, smallest, largest):
    def one(dim, parts):
        steps = jax.random.uniform(jax.random.fold_in(jax.random.fold_in(rng, 6), dim), (parts,), jnp.float32, smallest / len(shards), largest / len(shards))
        return jnp.repeat(jnp.exp(steps), extent[dim] // parts).reshape((-1,) + (1,) * (len(extent) - dim - 1))

    loudness = one(*shards[0])
    for cut in shards[1:]:
        loudness = loudness * one(*cut)
    return loudness


def profile(amount, total, most, skew):
    portions = [(1 << 20) // math.isqrt(grade ** skew) + 1 for grade in range(2, amount + 1)]
    rest, given = total - most - (amount - 1), [1] * (amount - 1)
    while rest > 0:
        free = [i for i in range(amount - 1) if given[i] < most]
        whole, left = sum([portions[i] for i in free]), rest
        for i in free:
            more = min(most - given[i], max(1, left * portions[i] // whole), rest)
            given[i] = given[i] + more
            rest = rest - more
    return np.array([most] + given)


def uneven(stream_key, count, total, reach, lean):
    if count == 2:
        one = jax.random.randint(stream_key, (), max(1, total - reach), min(reach, total - 1) + 1)
        return jnp.stack([one, total - one])
    sizes = jnp.asarray(profile(count, total, reach, lean), jnp.int32)
    couples = (count - 1) // 2
    giver, receiver = sizes[1:1 + 2 * couples:2], sizes[2:2 + 2 * couples:2]
    slack = jnp.minimum(giver - 1, reach - receiver)
    shifted = jax.random.randint(jax.random.fold_in(stream_key, 1), (couples,), 0, 1 << 20) % (slack + 1)
    sizes = sizes.at[1:1 + 2 * couples:2].set(giver - shifted).at[2:2 + 2 * couples:2].set(receiver + shifted)
    return sizes[jax.random.permutation(jax.random.fold_in(stream_key, 2), count)]


def shared_out(stream_key, own, number, rows, count, top, limit, slope):
    ranking = jax.random.permutation(stream_key, count)
    packed, ordinary = portions_of(count, rows * top, limit, slope, True), portions_of(count, rows * top, limit, slope, False)
    places = jnp.arange(count)

    def named(lengths, offset_by):
        used = int((lengths > 0).sum())
        fixed = max(1, used // 4)
        moved = fixed + (places - fixed + offset_by * (used - fixed)) % max(1, count - fixed)
        return jnp.zeros((count,), jnp.int32).at[ranking[jnp.where(places < fixed, places, moved)]].set(jnp.asarray(lengths, jnp.int32))

    lengths = jnp.where(number % 4 == 0, named(packed, number // 4), named(ordinary, number - number // 4 - 1))
    mixed = jax.random.permutation(jax.random.fold_in(own, 3), count)
    giver, taker = mixed[0:count // 2 * 2:2], mixed[1:count // 2 * 2:2]
    slack = jnp.minimum(lengths[giver] - 1, limit - lengths[taker]) // 2
    slack = jnp.where((giver == ranking[0]) | (taker == ranking[0]) | (lengths[taker] == 0), 0, jnp.maximum(slack, 0))
    moved = jax.random.randint(jax.random.fold_in(own, 4), (count // 2,), 0, 1 << 20) % (slack + 1)
    lengths = lengths.at[giver].add(-moved).at[taker].add(moved)
    members = jnp.searchsorted(jnp.cumsum(lengths), jnp.arange(rows * top), side="right").astype(jnp.int32)
    table = members.reshape(top, rows).T
    table = table[jax.random.permutation(jax.random.fold_in(own, 1), rows)]
    offset_by = jax.random.randint(jax.random.fold_in(own, 2), (rows, 1), 0, top)
    return jnp.take_along_axis(table, (jnp.arange(top)[None, :] + offset_by) % top, axis=1)


def portions_of(number_of, total, most, lean, full):
    portions = [(1 << 20) // math.isqrt(grade ** lean) + 1 for grade in range(1, number_of + 1)]
    largest = most if full else min(most, max(-(-total // number_of), total * portions[0] // sum(portions)))
    least = 1 if total - largest >= number_of - 1 else 0
    counts, spare = [largest] + [least] * (number_of - 1), total - largest - least * (number_of - 1)
    while spare > 0:
        movable = [i for i in range(1, number_of) if counts[i] < largest] or [i for i in range(1, number_of) if counts[i] < most]
        mass, remaining = sum([portions[i] for i in movable]), spare
        for i in movable:
            addition = min(most - counts[i], max(1, remaining * portions[i] // mass), spare)
            counts[i] = counts[i] + addition
            spare = spare - addition
    return np.array(counts)


def centred(key, dims, width, most, cuts=(), kind=jnp.bfloat16):
    values = width * jax.random.normal(key, dims, jnp.float32)
    if cuts:
        values = values * shard_levels(key, dims, cuts, -0.22, 0.18)
    return jnp.clip(values, -most, most).astype(kind)


def setup_inputs(seed: int = 0) -> dict:
    arg_keys = jax.random.split(jax.random.key(seed), 14)
    queries = draw_queries(jax.random.fold_in(arg_keys[13], 71), 0)
    keys = draw_keys(jax.random.fold_in(arg_keys[13], 71), 0)
    values = centred(arg_keys[2], (TEXT_SLOTS, KV_HEADS * HEAD_DIM), 1.0, 6.0, ((0, 64), (1, 4)))
    cum_gate = draw_cum_gate(jax.random.fold_in(arg_keys[13], 71), 0)
    doc_ids = jnp.searchsorted(jnp.cumsum(uneven(arg_keys[4], DOCS, TEXT_SLOTS, DOC_MOST, 0)), jnp.arange(TEXT_SLOTS), side="right").astype(jnp.int32)
    residual = centred(arg_keys[5], (TEXT_SLOTS, D), 1.0, 6.0, ((0, 256),))
    out_proj = centred(arg_keys[6], (ASKING_PLANES * HEAD_DIM, D), (ASKING_PLANES * HEAD_DIM) ** -0.5, 0.1875)
    norm_gain = jnp.clip(1.0 + 0.18 * jax.random.normal(arg_keys[7], (D,), jnp.float32), 0.1, 1.9)
    route_ids_keys = jax.random.split(jax.random.fold_in(arg_keys[8], 1), TEXT_SLOTS // ROWS_DEV)
    route_ids_turns = jax.random.permutation(jax.random.fold_in(arg_keys[8], 3), TEXT_SLOTS // ROWS_DEV)
    route_ids = jax.vmap(lambda own, number: shared_out(jax.random.fold_in(arg_keys[8], 2), own, number, ROWS_DEV, EXPERTS, TOP, CAP, 2))(route_ids_keys, route_ids_turns).reshape((TEXT_SLOTS, TOP))
    route_weights = jnp.clip(jnp.exp(math.log(1.0) - 1.609438 * jax.random.uniform(arg_keys[9], (TEXT_SLOTS, TOP), jnp.float32) ** shard_levels(arg_keys[9], (TEXT_SLOTS, TOP), ((0, 256),), -0.2, 0.2)), 0.2, 1.0)
    expert_gate = centred(arg_keys[10], (EXPERTS, D, EXPERT_FF), D ** -0.5, 0.125, ((0, 64), (2, 4)))
    expert_up = centred(arg_keys[11], (EXPERTS, D, EXPERT_FF), D ** -0.5, 0.125, ((0, 64), (2, 4)))
    expert_down = centred(arg_keys[12], (EXPERTS, EXPERT_FF, D), EXPERT_FF ** -0.5, 0.1875, ((0, 64), (1, 4)))
    return dict(queries=queries, keys=keys, values=values, cum_gate=cum_gate, doc_ids=doc_ids, residual=residual, out_proj=out_proj, norm_gain=norm_gain, route_ids=route_ids, route_weights=route_weights, expert_gate=expert_gate, expert_up=expert_up, expert_down=expert_down)


def head_attention(query_head, key_head, value_head, gate_head, doc_ids):
    qblock = math.gcd(TEXT_SLOTS, 512)
    scale = HEAD_DIM ** (-0.5)
    positions = jnp.arange(TEXT_SLOTS, dtype=jnp.int32)

    def one_block(index):
        first = index * qblock
        query_rows = lax.dynamic_slice_in_dim(query_head, first, qblock, 0)
        gate_rows = lax.dynamic_slice_in_dim(gate_head, first, qblock, 0)
        doc_rows = lax.dynamic_slice_in_dim(doc_ids, first, qblock, 0)
        query_pos = first + jnp.arange(qblock, dtype=jnp.int32)
        scores = jnp.dot(query_rows, key_head.T, preferred_element_type=jnp.float32) * scale
        scores = scores + gate_rows[:, None] - gate_head[None, :]
        allowed = (positions[None, :] <= query_pos[:, None]) & (doc_ids[None, :] == doc_rows[:, None])
        scores = jnp.where(allowed, scores, -jnp.inf)
        top = lax.optimization_barrier(jnp.max(scores, axis=1, keepdims=True))
        expo = jnp.exp(scores - top)
        total = lax.optimization_barrier(jnp.sum(expo, axis=1, keepdims=True))
        summed = jnp.dot(expo.astype(jnp.bfloat16), value_head, preferred_element_type=jnp.float32)
        return (summed / total).astype(jnp.bfloat16)
    blocks = lax.map(one_block, jnp.arange(TEXT_SLOTS // qblock, dtype=jnp.int32))
    return blocks.reshape(TEXT_SLOTS, HEAD_DIM)

def reference(queries, keys, values, cum_gate, doc_ids, residual, out_proj, norm_gain, route_ids, route_weights, expert_gate, expert_up, expert_down):
    group_size = ASKING_PLANES // KV_HEADS
    query_heads = queries.reshape(TEXT_SLOTS, ASKING_PLANES, HEAD_DIM).transpose(1, 0, 2)
    key_heads = keys.reshape(TEXT_SLOTS, KV_HEADS, HEAD_DIM).transpose(1, 0, 2)
    value_heads = values.reshape(TEXT_SLOTS, KV_HEADS, HEAD_DIM).transpose(1, 0, 2)
    gate_heads = cum_gate.T
    owner = jnp.arange(ASKING_PLANES, dtype=jnp.int32) // group_size

    def per_head(inputs):
        query_head, gate_head, kv_index = inputs
        return head_attention(query_head, key_heads[kv_index], value_heads[kv_index], gate_head, doc_ids)
    attended = lax.map(per_head, (query_heads, gate_heads, owner))
    attended = attended.transpose(1, 0, 2).reshape(TEXT_SLOTS, ASKING_PLANES * HEAD_DIM)
    projected = jnp.dot(attended, out_proj, preferred_element_type=jnp.float32)
    stream = (residual.astype(jnp.float32) + projected).astype(jnp.bfloat16)
    stream_f = stream.astype(jnp.float32)
    normed = stream_f * lax.rsqrt(lax.optimization_barrier(jnp.mean(stream_f * stream_f, axis=1, keepdims=True)) + 1e-06)
    normed = (normed * norm_gain[None, :]).astype(jnp.bfloat16)
    block_count = TEXT_SLOTS // ROWS_DEV
    flat = route_ids.reshape(block_count, ROWS_DEV * TOP)
    onehot = (flat[..., None] == jnp.arange(EXPERTS, dtype=jnp.int32)).astype(jnp.int32)
    earlier = jnp.cumsum(onehot, axis=1) - onehot
    rank = lax.optimization_barrier(jnp.sum(earlier * onehot, axis=2))
    per_expert = block_count * CAP
    block_index = jnp.arange(block_count, dtype=jnp.int32)[:, None]
    slot = (flat * per_expert + block_index * CAP + rank).reshape(-1)
    token_of = jnp.arange(TEXT_SLOTS * TOP, dtype=jnp.int32) // TOP
    table = jnp.full((EXPERTS * per_expert,), TEXT_SLOTS, jnp.int32).at[slot].set(token_of)
    weight_table = jnp.zeros((EXPERTS * per_expert,), jnp.float32).at[slot].set(route_weights.reshape(-1))
    padded = jnp.concatenate([normed, jnp.zeros((1, D), jnp.bfloat16)], axis=0)
    quarter = EXPERT_FF // N_TP

    def one_expert(accum, inputs):
        index_rows, weight_rows, gate_weight, up_w, down_w = inputs
        rows = padded[index_rows]
        gate = jnp.dot(rows, gate_weight, preferred_element_type=jnp.float32)
        upper = jnp.dot(rows, up_w, preferred_element_type=jnp.float32)
        hidden = (jax.nn.silu(gate) * upper).astype(jnp.bfloat16)
        hidden_groups = hidden.reshape(per_expert, N_TP, quarter).astype(jnp.float32)
        down_groups = down_w.reshape(N_TP, quarter, D).astype(jnp.float32)
        pieces = jnp.einsum('rgf,gfd->grd', hidden_groups, down_groups).astype(jnp.bfloat16)
        pieces = lax.optimization_barrier(pieces)
        expert_out = lax.optimization_barrier(jnp.sum(pieces.astype(jnp.float32), axis=0)).astype(jnp.bfloat16)
        accum = accum.at[index_rows].add(weight_rows[:, None] * expert_out.astype(jnp.float32))
        return (accum, None)
    accum, _ = lax.scan(one_expert, jnp.zeros((TEXT_SLOTS + 1, D), jnp.float32), (table.reshape(EXPERTS, per_expert), weight_table.reshape(EXPERTS, per_expert), expert_gate, expert_up, expert_down))
    return (stream_f + accum[:TEXT_SLOTS]).astype(jnp.bfloat16)
```

```python
import functools

import jax
import jax.numpy as jnp
from jax import lax
from jax.experimental import pallas as pl
from jax.experimental.pallas import tpu as pltpu
from jax.sharding import PartitionSpec as P

MESH = pl.DeviceIdType.MESH
F32, BF16 = jnp.float32, jnp.bfloat16

D = 2048
HEAD_DIM = 64
NZ, NX, NC, NT = 8, 4, 2, 4
PLANE = NX * NC
TOK = 128
HEADS = 4
ROWS = 32
BLK = 144
BACK = 4
WIDE = 256
PIECES = D // WIDE
very_low = -1e30
norm_eps = 1e-06


def at(sp, tp):
    return {"sp": sp, "tp": tp}


def remote(src, dst, send, recv, sp, tp):
    return pltpu.make_async_remote_copy(
        src_ref=src, dst_ref=dst, send_sem=send, recv_sem=recv, device_id=at(sp, tp), device_id_type=MESH
    )


def index_of(z, x, c):
    return ((z + NZ) % NZ * NX + (x + NX) % NX) * NC + (c + NC) % NC


def place():
    sp, tp = lax.axis_index("sp"), lax.axis_index("tp")
    return sp, tp, sp // PLANE, sp // NC % NX, sp % NC


def attention_kernel(
    q_ref, k_ref, v_ref, gate_ref, doc_ref, res_ref, gain_ref, proj_hbm,
    stream_ref, stacked_ref,
    kvg, aux, qs, bias, top, acc, att, planes, proj,
    recv, send, arecv, asend, psem,
):
    sp, tp, z, x, c = place()
    load = pltpu.make_async_copy(proj_hbm, proj, psem)
    load.start()

    barrier = pltpu.get_barrier_semaphore()
    partners = [
        index_of(z + 1, x, c), index_of(z - 1, x, c), index_of(z + 2, x, c), index_of(z - 2, x, c),
        index_of(z, x + 1, c), index_of(z, x + 3, c), index_of(z, x + 2, c), index_of(z, x, c + 1),
        index_of(z + 5, x + 1, c + 1), index_of(z - 5, x + 3, c + 1),
    ]
    for other in partners:
        pl.semaphore_signal(barrier, inc=1, device_id=at(other, tp), device_id_type=MESH)
    for step in range(1, NT):
        pl.semaphore_signal(barrier, inc=1, device_id=at(sp, (tp + step) % NT), device_id_type=MESH)

    kvg[sp, 0:HEAD_DIM, :] = k_ref[...]
    kvg[sp, HEAD_DIM : 2 * HEAD_DIM, :] = v_ref[...]
    aux[...] = jnp.zeros_like(aux)
    aux[0:HEADS, :] = gate_ref[...]
    aux[HEADS : HEADS + 1, :] = doc_ref[...].astype(F32)
    own = aux[...]
    high = own.astype(BF16).astype(F32)
    rest = own - high
    mid = rest.astype(BF16).astype(F32)
    low = rest - mid
    sub = lax.broadcasted_iota(jnp.int32, (8, TOK), 0)
    first = jnp.where(sub < HEADS, high, pltpu.roll(mid, HEADS, 0))
    second = jnp.where(sub < HEADS, low, own)
    kvg[sp, 2 * HEAD_DIM : BLK, :] = jnp.concatenate([first, second], axis=0).astype(BF16)

    lane = lax.broadcasted_iota(jnp.int32, (TOK, TOK), 1)
    for pair in range(HEADS // 2):
        both = q_ref[:, pair * TOK : (pair + 1) * TOK].astype(F32) * (HEAD_DIM**-0.5)
        for half in range(2):
            turned = both if half == 0 else pltpu.roll(both, HEAD_DIM, 1)
            qs[pl.ds((pair * 2 + half) * TOK, TOK), :] = jnp.where(lane < HEAD_DIM, turned, 0.0).astype(BF16)
    query_doc = jnp.broadcast_to(own[HEADS : HEADS + 1, :], (TOK, TOK)).T
    top[...] = jnp.full_like(top, very_low)
    acc[...] = jnp.zeros_like(acc)

    pl.semaphore_wait(barrier, len(partners) + NT - 1)

    def push(slot, target):
        remote(kvg.at[slot], kvg.at[slot], send, recv.at[slot], target, tp).start()

    def arrived(slot):
        remote(kvg.at[slot], kvg.at[slot], send, recv.at[slot], sp, (tp + 1) % NT).wait_recv()

    def spread(slot):
        push(slot, index_of(z, x + 1, c))
        push(slot, index_of(z, x + 3, c))
        push(slot, index_of(z, x + 2, c))
        push(slot, index_of(z, x, c + 1))

    def across(back):
        for step in (1, 3, 2):
            slot = index_of(z - back, x + step, c)
            arrived(slot)
            push(slot, index_of(z, x, c + 1))

    def beside(back):
        for step in range(NX):
            arrived(index_of(z - back, x + step, c + 1))

    extra = index_of(z - 5, x + 3, c + 1)
    extra_off = jnp.where((x == 0) & (c == 0) & (z >= 5), 0.0, -64.0)

    def attend(back):
        plane = (z - back + NZ) % NZ
        slots = [plane * PLANE + k for k in range(PLANE)]
        off = jnp.where(z >= back, 0.0, -64.0)
        offs = [off] * PLANE
        if back == BACK:
            slots.append(extra)
            offs.append(extra_off)
        width = len(slots) * TOK
        gate_first = own[:, 0:1]
        row8 = lax.broadcasted_iota(jnp.int32, (8, TOK), 0)
        blocks = []
        for k, (slot, shift) in enumerate(zip(slots, offs)):
            parts = kvg[slot, 2 * HEAD_DIM : BLK, :].astype(F32)
            upper, lower = parts[0:8], parts[8:16]
            gates = gate_first - (upper + pltpu.roll(upper, HEADS, 0) + lower)
            bias[:, k * TOK : (k + 1) * TOK] = jnp.where(row8 < HEADS, gates, lower + shift)
            blocks.append(kvg[slot, 0 : 2 * HEAD_DIM, :])
        kv = jnp.concatenate(blocks, axis=1)
        row = lax.broadcasted_iota(jnp.int32, kv.shape, 0)
        ones_v = jnp.where(row < HEAD_DIM, jnp.ones_like(kv), kv)
        allowed = jnp.concatenate([query_doc] * len(slots), axis=1) == bias[HEADS : HEADS + 1, 0:width]
        if back == 0:
            key_pos = lax.broadcasted_iota(jnp.int32, (TOK, width), 1)
            query_pos = lax.broadcasted_iota(jnp.int32, (TOK, width), 0) + (x * NC + c) * TOK
            allowed = allowed & (key_pos <= query_pos)
        for head in range(HEADS):
            rows = slice(head * TOK, (head + 1) * TOK)
            scores = jnp.dot(qs[rows, :], kv, preferred_element_type=F32)
            scores = jnp.where(allowed, scores + bias[head : head + 1, 0:width], very_low)
            top_old = top[rows, :]
            top_new = jnp.maximum(top_old, jnp.max(scores, axis=1, keepdims=True))
            weights = jnp.exp(scores - top_new[:, 0:1]).astype(BF16)
            part = lax.dot_general(
                weights, ones_v, (((1,), (1,)), ((), ())), preferred_element_type=F32
            )
            acc[rows, :] = acc[rows, :] * jnp.exp(top_old - top_new) + part
            top[rows, :] = top_new

    one, two, three, four = (index_of(z - back, x, c) for back in (1, 2, 3, 4))
    push(sp, index_of(z + 1, x, c))
    push(sp, index_of(z + 2, x, c))
    spread(sp)
    push(sp, index_of(z + 5, x + 1, c + 1))
    arrived(one)
    spread(one)
    arrived(two)
    push(two, index_of(z + 1, x, c))
    push(two, index_of(z + 2, x, c))
    spread(two)
    across(0)
    across(1)
    beside(0)
    attend(0)
    arrived(three)
    spread(three)
    across(2)
    beside(1)
    attend(1)
    arrived(four)
    spread(four)
    across(3)
    beside(2)
    attend(2)
    across(4)
    beside(3)
    attend(3)
    beside(4)
    arrived(extra)
    attend(4)

    done = []
    for head in range(HEADS):
        summed = acc[head * TOK : (head + 1) * TOK, :]
        done.append(summed / pltpu.roll(summed, HEAD_DIM, 1))
    for pair in range(HEADS // 2):
        left = pltpu.roll(done[2 * pair], HEAD_DIM, 1)
        att[:, pair * TOK : (pair + 1) * TOK] = jnp.where(lane < HEAD_DIM, left, done[2 * pair + 1]).astype(BF16)
    for step in (1, 3, 2):
        other = (tp + step) % NT
        remote(
            att.at[pl.ds(pl.multiple_of(other * ROWS, ROWS), ROWS)], planes.at[tp], asend, arecv.at[tp], sp, other
        ).start()
    load.wait()
    depth = HEADS * HEAD_DIM

    def part_of(rows, group):
        weights = proj[pl.ds(pl.multiple_of(group * depth, depth), depth), :]
        return jnp.dot(rows, weights, preferred_element_type=F32)

    total = part_of(att[pl.ds(pl.multiple_of(tp * ROWS, ROWS), ROWS), :], tp)
    for step in (1, 3, 2):
        other = (tp + step) % NT
        remote(planes.at[other], planes.at[other], asend, arecv.at[other], sp, other).wait_recv()
        total = total + part_of(planes[other], other)
    stream = (res_ref[...].astype(F32) + total).astype(BF16)
    stream_ref[...] = stream
    stream = stream.astype(F32)
    normed = stream * lax.rsqrt(jnp.mean(stream * stream, axis=1, keepdims=True) + norm_eps)
    normed = (normed * gain_ref[...]).astype(BF16)
    for piece in range(PIECES):
        stacked_ref[piece * ROWS : (piece + 1) * ROWS, :] = normed[:, piece * WIDE : (piece + 1) * WIDE]

    count = 5 + 15 + 20
    remote(kvg.at[pl.ds(0, count)], kvg.at[pl.ds(0, count)], send, recv.at[0], sp, (tp + 1) % NT).wait_send()
    remote(planes.at[pl.ds(0, 3)], planes.at[pl.ds(0, 3)], asend, arecv.at[0], sp, (tp + 1) % NT).wait_send()


def expert_kernel(
    stacked_ref, stream_ref, ids_ref, weights_ref, gate_hbm, up_hbm, down_hbm,
    out_ref,
    turn, choose, sent, came, pick, xrows, w_gate, w_up, w_down,
    pieces, half_l, half_r, full_l, full_r, to_r, to_l, back, final,
    wsem, dsend, drecv, ysend, yl, yr, ya, yb, rsend, ra, rb, rl, rr, fsend, frecv,
):
    sp, tp, z, x, c = place()
    own_in_plane = x * NC + c
    right, left, far = (tp + 1) % NT, (tp + 3) % NT, (tp + 2) % NT
    experts = NZ * PLANE
    loads = [
        pltpu.make_async_copy(hbm.at[0], vmem, wsem.at[k])
        for k, (hbm, vmem) in enumerate(((gate_hbm, w_gate), (up_hbm, w_up), (down_hbm, w_down)))
    ]
    for load in loads:
        load.start()

    barrier = pltpu.get_barrier_semaphore()

    def greet(step, carry):
        pl.semaphore_signal(barrier, inc=1, device_id=at((sp + step) % experts, tp), device_id_type=MESH)
        return carry

    lax.fori_loop(1, experts, greet, 0)
    for step in range(1, NT):
        pl.semaphore_signal(barrier, inc=1, device_id=at(sp, (tp + step) % NT), device_id_type=MESH)

    def plane_at(g):
        away = (g + 1) // 2 * (1 - 2 * ((g + 1) % 2))
        return (z + away + NZ) % NZ

    turn[...] = jnp.zeros_like(turn)
    turn[0:2, 0:ROWS] = ids_ref[...].astype(F32)
    turn[2:4, 0:ROWS] = weights_ref[...]
    along = turn[0:8, 0:ROWS]
    columns = turn[...].T[0:ROWS, :]
    low = lax.broadcasted_iota(jnp.int32, (ROWS, ROWS), 0)
    high = lax.broadcasted_iota(jnp.int32, (ROWS, ROWS), 1)
    lane = lax.broadcasted_iota(jnp.int32, (ROWS, 2 * WIDE), 1)
    spread = jnp.where(
        lax.broadcasted_iota(jnp.int32, (ROWS, WIDE), 1) % ROWS == lax.broadcasted_iota(jnp.int32, (ROWS, WIDE), 0),
        1.0, 0.0,
    ).astype(BF16)
    piece_of = (lax.broadcasted_iota(jnp.int32, (8, WIDE), 1) // ROWS).astype(F32)
    targets = []
    for k in range(2):
        line, column = along[k : k + 1, :], columns[:, k : k + 1]
        rank_line = jnp.zeros((1, ROWS), F32)
        rank_column = jnp.zeros((ROWS, 1), F32)
        for other in range(2):
            same = (columns[:, other : other + 1] == line) & (low < high)
            rank_line = rank_line + jnp.sum(jnp.where(same, 1.0, 0.0), axis=0, keepdims=True)
            same = (along[other : other + 1, :] == column) & (high < low)
            rank_column = rank_column + jnp.sum(jnp.where(same, 1.0, 0.0), axis=1, keepdims=True)
        slot = jnp.broadcast_to(line * 2.0 + rank_line, (8, ROWS)).astype(BF16)
        targets.append(jnp.dot(slot, spread, preferred_element_type=F32) * PIECES + piece_of)
        base = (column * 2.0 + rank_column) * PIECES
        for piece in range(PIECES):
            want = (base + piece).astype(jnp.int32)
            for plane in range(NZ):
                spots = lax.broadcasted_iota(jnp.int32, (ROWS, TOK), 1) + plane * TOK
                rows = slice((k * PIECES + piece) * ROWS, (k * PIECES + piece + 1) * ROWS)
                pick[plane, rows, :] = jnp.where(spots == want, 1.0, 0.0).astype(BF16)
    spots = lax.broadcasted_iota(jnp.int32, (experts * 16, WIDE), 0)
    hit = (spots == targets[0][0:1, :].astype(jnp.int32)) | (spots == targets[1][0:1, :].astype(jnp.int32))
    chosen = jnp.where(hit, 1.0, 0.0).astype(BF16)
    sent[...] = (
        jnp.dot(chosen, stacked_ref[...], preferred_element_type=F32).astype(BF16).reshape(experts, 16, WIDE)
    )
    src = lax.broadcasted_iota(jnp.int32, (TOK, TOK), 0)
    dst = lax.broadcasted_iota(jnp.int32, (TOK, TOK), 1)
    choose[0] = jnp.where((dst // 8 == src % 16) & (dst % 8 == src // 16), 1.0, 0.0).astype(BF16)
    choose[1] = jnp.where((src // 8 == dst % 16) & (src % 8 == dst // 16), 1.0, 0.0).astype(BF16)

    pl.semaphore_wait(barrier, experts - 1 + NT - 1)

    def dispatch(g, carry):
        plane = plane_at(g)

        def one(k, inner):
            target = plane * PLANE + k

            @pl.when(target != sp)
            def _():
                remote(sent.at[target], came.at[tp, sp], dsend, drecv.at[z], target, tp).start()

            @pl.when(target == sp)
            def _():
                pltpu.make_async_copy(sent.at[sp], came.at[tp, sp], drecv.at[z]).start()

            return inner

        return lax.fori_loop(0, PLANE, one, carry)

    lax.fori_loop(0, NZ, dispatch, 0)

    def group(ref, source, plane, half=None):
        if half is None:
            return ref.at[source, pl.ds(pl.multiple_of(plane * PLANE, PLANE), PLANE)]
        return ref.at[source, pl.ds(pl.multiple_of(plane * PLANE + half * (PLANE // 2), PLANE // 2), PLANE // 2)]

    def share(g):
        plane = plane_at(g)
        ref = group(came, tp, plane)
        remote(ref, ref, dsend, drecv.at[plane], sp, right).wait_recv()
        remote(ref, ref, ysend, yl.at[g], sp, right).start()
        remote(ref, ref, ysend, yr.at[g], sp, left).start()

    def relay(g):
        plane = plane_at(g)
        ref = group(came, left, plane)
        remote(ref, ref, ysend, yl.at[g], sp, right).wait_recv()
        ref = group(came, left, plane, 0)
        remote(ref, ref, ysend, ya.at[g], sp, right).start()
        ref = group(came, right, plane)
        remote(ref, ref, ysend, yr.at[g], sp, left).wait_recv()
        ref = group(came, right, plane, 1)
        remote(ref, ref, ysend, yb.at[g], sp, left).start()

    def gathered(g):
        plane = plane_at(g)
        ref = group(came, far, plane, 0)
        remote(ref, ref, ysend, ya.at[g], sp, right).wait_recv()
        ref = group(came, far, plane, 1)
        remote(ref, ref, ysend, yb.at[g], sp, right).wait_recv()

    def compute(chunk):
        for k in range(2):
            plane = plane_at(2 * chunk + k)
            for source in range(NT):
                rows = came[source, pl.ds(pl.multiple_of(plane * PLANE, PLANE), PLANE)].reshape(TOK, WIDE)
                ordered = jnp.dot(choose[0], rows, preferred_element_type=F32).astype(BF16)
                q = (k * NT + source) * 16
                for piece in range(PIECES):
                    xrows[q : q + 16, piece * WIDE : (piece + 1) * WIDE] = ordered[piece * 16 : piece * 16 + 16, :]
        rows = xrows[...]
        gate = jnp.dot(rows, w_gate[...], preferred_element_type=F32)
        upper = jnp.dot(rows, w_up[...], preferred_element_type=F32)
        hidden = (gate / (1.0 + jnp.exp(-gate)) * upper).astype(BF16)
        part = jnp.dot(hidden, w_down[...], preferred_element_type=F32).astype(BF16)
        for k in range(2):
            for source in range(NT):
                q = (k * NT + source) * 16
                pieces[2 * chunk + k, source] = part[q : q + 16, :]

    half = D // 2

    def first_halves(g):
        remote(pieces.at[g, far, :, pl.ds(0, half)], half_l.at[g], rsend, ra.at[g], sp, right).start()
        remote(pieces.at[g, far, :, pl.ds(half, half)], half_r.at[g], rsend, rb.at[g], sp, left).start()

    def add_half(g):
        remote(half_l.at[g], half_l.at[g], rsend, ra.at[g], sp, right).wait_recv()
        mine = pieces[g, right]
        to_r[g, :, 0:half] = (mine[:, 0:half].astype(F32) + half_l[g].astype(F32)).astype(BF16)
        to_r[g, :, half:] = mine[:, half:]
        remote(to_r.at[g], full_l.at[g], rsend, rl.at[g], sp, right).start()
        remote(half_r.at[g], half_r.at[g], rsend, rb.at[g], sp, right).wait_recv()
        mine = pieces[g, left]
        to_l[g, :, half:] = (mine[:, half:].astype(F32) + half_r[g].astype(F32)).astype(BF16)
        to_l[g, :, 0:half] = mine[:, 0:half]
        remote(to_l.at[g], full_r.at[g], rsend, rr.at[g], sp, left).start()

    def give_back(g):
        plane = plane_at(g)
        remote(full_l.at[g], full_l.at[g], rsend, rl.at[g], sp, right).wait_recv()
        remote(full_r.at[g], full_r.at[g], rsend, rr.at[g], sp, right).wait_recv()
        total = pieces[g, tp].astype(F32) + full_l[g].astype(F32) + full_r[g].astype(F32)
        total = total.astype(BF16)
        stacked = jnp.concatenate([total[:, k * WIDE : (k + 1) * WIDE] for k in range(PIECES)], axis=0)
        mixed = jnp.dot(choose[1], stacked, preferred_element_type=F32).astype(BF16)
        back[pl.ds(pl.multiple_of(g * PLANE, PLANE), PLANE)] = mixed.reshape(PLANE, 16, WIDE)

        def one(k, carry):
            target = plane * PLANE + k

            @pl.when(target != sp)
            def _():
                remote(back.at[g * PLANE + k], final.at[sp], fsend, frecv.at[z], target, tp).start()

            @pl.when(target == sp)
            def _():
                pltpu.make_async_copy(back.at[g * PLANE + k], final.at[sp], frecv.at[z]).start()

            return carry

        lax.fori_loop(0, PLANE, one, 0)

    chunks = NZ // 2
    share(0)
    share(1)
    for load in loads:
        load.wait()

    def step(chunk, carry):
        relay(2 * chunk)

        @pl.when(chunk < chunks - 1)
        def _():
            share(2 * chunk + 2)

        relay(2 * chunk + 1)

        @pl.when(chunk < chunks - 1)
        def _():
            share(2 * chunk + 3)

        @pl.when(chunk > 0)
        def _():
            add_half(2 * chunk - 2)
            add_half(2 * chunk - 1)

        @pl.when(chunk > 1)
        def _():
            give_back(2 * chunk - 4)
            give_back(2 * chunk - 3)

        gathered(2 * chunk)
        gathered(2 * chunk + 1)
        compute(chunk)
        first_halves(2 * chunk)
        first_halves(2 * chunk + 1)
        return carry

    lax.fori_loop(0, chunks, step, 0)
    give_back(NZ - 4)
    give_back(NZ - 3)
    add_half(NZ - 2)
    add_half(NZ - 1)
    give_back(NZ - 2)
    give_back(NZ - 1)

    def take(g, total):
        plane = plane_at(g)
        ref = final.at[pl.ds(pl.multiple_of(plane * PLANE, PLANE), PLANE)]
        remote(ref, ref, fsend, frecv.at[plane], sp, right).wait_recv()
        rows = final[pl.ds(pl.multiple_of(plane * PLANE, PLANE), PLANE)].reshape(TOK, WIDE)
        return total + jnp.dot(pick[plane], rows, preferred_element_type=F32)

    total = lax.fori_loop(0, NZ, take, jnp.zeros((2 * PIECES * ROWS, WIDE), F32))
    weight0, weight1 = columns[:, 2:3], columns[:, 3:4]
    for piece in range(PIECES):
        lanes = slice(piece * WIDE, (piece + 1) * WIDE)
        one = total[piece * ROWS : (piece + 1) * ROWS]
        two = total[(PIECES + piece) * ROWS : (PIECES + piece + 1) * ROWS]
        out_ref[:, lanes] = (stream_ref[:, lanes].astype(F32) + (weight0 * one + weight1 * two)).astype(BF16)

    some = sent.at[pl.ds(0, experts - 1)]
    remote(some, some, dsend, drecv.at[0], sp, right).wait_send()
    some = came.at[pl.ds(0, 3)]
    remote(some, some, ysend, yl.at[0], sp, right).wait_send()
    some = pieces.at[pl.ds(0, 6)]
    remote(some, some, rsend, ra.at[0], sp, right).wait_send()
    some = final.at[pl.ds(0, experts - 1)]
    remote(some, some, fsend, frecv.at[0], sp, right).wait_send()


def local(
    queries, keys, values, cum_gate, doc_ids, residual, out_proj, norm_gain, route_ids, route_weights,
    expert_gate, expert_up, expert_down,
):
    vmem, anywhere = pl.BlockSpec(memory_space=pltpu.VMEM), pl.BlockSpec(memory_space=pl.ANY)
    dma, sds = pltpu.SemaphoreType.DMA, jax.ShapeDtypeStruct
    experts = NZ * PLANE
    stream, stacked = pl.pallas_call(
        attention_kernel,
        out_shape=(sds((ROWS, D), BF16), sds((PIECES * ROWS, WIDE), BF16)),
        in_specs=[vmem] * 7 + [anywhere],
        out_specs=(vmem, vmem),
        scratch_shapes=[
            pltpu.VMEM((experts, BLK, TOK), BF16),
            pltpu.VMEM((8, TOK), F32),
            pltpu.VMEM((HEADS * TOK, TOK), BF16),
            pltpu.VMEM((8, (PLANE + 1) * TOK), F32),
            pltpu.VMEM((HEADS * TOK, TOK), F32),
            pltpu.VMEM((HEADS * TOK, TOK), F32),
            pltpu.VMEM((TOK, HEADS * HEAD_DIM), BF16),
            pltpu.VMEM((NT, ROWS, HEADS * HEAD_DIM), BF16),
            pltpu.VMEM((NT * HEADS * HEAD_DIM, D), BF16),
            dma((experts,)), dma, dma((NT,)), dma, dma,
        ],
        compiler_params=pltpu.CompilerParams(
            collective_id=0, has_side_effects=True, vmem_limit_bytes=50 << 20
        ),
        name="attention",
    )(queries, keys.T, values.T, cum_gate.T, doc_ids[None], residual, norm_gain[None], out_proj)
    return pl.pallas_call(
        expert_kernel,
        out_shape=sds((ROWS, D), BF16),
        in_specs=[vmem] * 4 + [anywhere] * 3,
        out_specs=vmem,
        scratch_shapes=[
            pltpu.VMEM((TOK, TOK), F32),
            pltpu.VMEM((2, TOK, TOK), BF16),
            pltpu.VMEM((experts, 16, WIDE), BF16),
            pltpu.VMEM((NT, experts, 16, WIDE), BF16),
            pltpu.VMEM((NZ, 2 * PIECES * ROWS, TOK), BF16),
            pltpu.VMEM((TOK, D), BF16),
            pltpu.VMEM((D, WIDE), BF16),
            pltpu.VMEM((D, WIDE), BF16),
            pltpu.VMEM((WIDE, D), BF16),
            pltpu.VMEM((NZ, NT, 16, D), BF16),
            pltpu.VMEM((NZ, 16, D // 2), BF16),
            pltpu.VMEM((NZ, 16, D // 2), BF16),
            pltpu.VMEM((NZ, 16, D), BF16),
            pltpu.VMEM((NZ, 16, D), BF16),
            pltpu.VMEM((NZ, 16, D), BF16),
            pltpu.VMEM((NZ, 16, D), BF16),
            pltpu.VMEM((experts, 16, WIDE), BF16),
            pltpu.VMEM((experts, 16, WIDE), BF16),
            dma((3,)), dma, dma((NZ,)), dma, dma((NZ,)), dma((NZ,)), dma((NZ,)), dma((NZ,)),
            dma, dma((NZ,)), dma((NZ,)), dma((NZ,)), dma((NZ,)), dma, dma((NZ,)),
        ],
        compiler_params=pltpu.CompilerParams(
            collective_id=1, has_side_effects=True, vmem_limit_bytes=50 << 20
        ),
        name="experts",
    )(stacked, stream, route_ids.T, route_weights.T, expert_gate, expert_up, expert_down)


def solution(mesh):
    in_specs = (
        P("sp", "tp"),
        P("sp", "tp"),
        P("sp", "tp"),
        P("sp", "tp"),
        P("sp"),
        P(("sp", "tp"), None),
        P(),
        P(),
        P(("sp", "tp"), None),
        P(("sp", "tp"), None),
        P("sp", None, "tp"),
        P("sp", None, "tp"),
        P("sp", "tp", None),
    )
    out_specs = P(("sp", "tp"), None)
    return jax.shard_map(local, mesh=mesh, in_specs=in_specs, out_specs=out_specs, check_vma=False)
```

```python
import functools

import jax
import jax.numpy as jnp
from jax import lax
from jax.experimental import pallas as pl
from jax.experimental.pallas import tpu as pltpu
from jax.sharding import PartitionSpec as P

MESH = pl.DeviceIdType.MESH
F32, BF16 = jnp.float32, jnp.bfloat16

D = 2048
HEAD_DIM = 64
NZ, NX, NC, NT = 8, 4, 2, 4
PLANE = NX * NC
TOK = 128
HEADS = 4
ROWS = 32
BLK = 144
BACK = 4
WIDE = 256
PIECES = D // WIDE
AHEAD = 4
ORDER = (0, 1, -3, 3, 4, -2, 2, -1)
very_low = -1e30
norm_eps = 1e-06


def at(sp, tp):
    return {"sp": sp, "tp": tp}


def remote(src, dst, send, recv, sp, tp):
    return pltpu.make_async_remote_copy(
        src_ref=src, dst_ref=dst, send_sem=send, recv_sem=recv, device_id=at(sp, tp), device_id_type=MESH
    )


def index_of(z, x, c):
    return ((z + NZ) % NZ * NX + (x + NX) % NX) * NC + (c + NC) % NC


def place():
    sp, tp = lax.axis_index("sp"), lax.axis_index("tp")
    return sp, tp, sp // PLANE, sp // NC % NX, sp % NC


def layer_kernel(
    q_hbm, k_hbm, v_hbm, gates_hbm, doc_hbm, res_hbm, gain_hbm, proj_hbm,
    ids_hbm, weights_hbm, gate_hbm, up_hbm, down_hbm,
    out_ref,
    q_ref, gates_ref, doc_ref, res_ref, gain_ref, ids_ref, weights_ref,
    kvg, aux, qs, bias, top, acc, soft, turned_v, att, planes, proj, kept, stacked,
    turn, chosen, choose, sent, came, pick, xrows, w_gate, w_up, w_down,
    hidden, hid_out, hid_in, pieces, half_l, half_r, full_l, full_r, to_r, to_l, back, final,
    insem, recv, send, arecv, asend, psem,
    wsem, dsend, drecv, ysend, yl, yr, ya, yb, rsend, ra, rb, rl, rr, fsend, frecv,
    gsend, gl, gr, hsend, hrecv,
):
    sp, tp, z, x, c = place()
    right, left, far = (tp + 1) % NT, (tp + 3) % NT, (tp + 2) % NT
    experts = NZ * PLANE
    barrier = pltpu.get_barrier_semaphore()
    in_copies = {}
    for k, (name, hbm, vmem) in enumerate((
        ("k", k_hbm, kvg.at[sp, pl.ds(0, HEAD_DIM)]), ("v", v_hbm, kvg.at[sp, pl.ds(HEAD_DIM, HEAD_DIM)]),
        ("gates", gates_hbm, gates_ref), ("doc", doc_hbm, doc_ref), ("q", q_hbm, q_ref), ("ids", ids_hbm, ids_ref),
        ("weights", weights_hbm, weights_ref), ("res", res_hbm, res_ref), ("gain", gain_hbm, gain_ref),
    )):
        in_copies[name] = pltpu.make_async_copy(hbm, vmem, insem.at[k])
        in_copies[name].start()

    def greet(step, carry):
        pl.semaphore_signal(barrier, inc=1, device_id=at((sp + step) % experts, tp), device_id_type=MESH)
        return carry

    lax.fori_loop(1, experts, greet, 0)
    for step in range(1, NT):
        pl.semaphore_signal(barrier, inc=1, device_id=at(sp, (tp + step) % NT), device_id_type=MESH)
    load = pltpu.make_async_copy(proj_hbm, proj, psem)
    load.start()
    loads = [
        pltpu.make_async_copy(hbm.at[0], vmem, wsem.at[k])
        for k, (hbm, vmem) in enumerate(((down_hbm, w_down.at[tp]), (gate_hbm, w_gate), (up_hbm, w_up)))
    ]
    for load_w in loads:
        load_w.start()
    for name in ("k", "v", "gates", "doc", "q"):
        in_copies[name].wait()

    def part_down(source, part):
        return w_down.at[source, pl.ds(part * (WIDE // 2), WIDE // 2)]

    def share_down():
        loads[0].wait()
        for part in (0, 1):
            ref = part_down(tp, part)
            remote(ref, ref, gsend, gl.at[part], sp, right).start()
            ref = part_down(tp, 1 - part)
            remote(ref, ref, gsend, gr.at[1 - part], sp, left).start()

    def pass_down():
        ref = part_down(left, 0)
        remote(ref, ref, gsend, gl.at[0], sp, right).wait_recv()
        remote(ref, ref, gsend, gl.at[2], sp, right).start()
        ref = part_down(right, 1)
        remote(ref, ref, gsend, gr.at[1], sp, right).wait_recv()
        remote(ref, ref, gsend, gr.at[2], sp, left).start()

    def all_down():
        for source, part, sem in ((left, 1, gl.at[1]), (right, 0, gr.at[0]), (far, 0, gl.at[2]), (far, 1, gr.at[2])):
            ref = part_down(source, part)
            remote(ref, ref, gsend, sem, sp, right).wait_recv()

    aux[...] = jnp.zeros_like(aux)
    aux[0:HEADS, :] = gates_ref[...]
    aux[HEADS : HEADS + 1, :] = doc_ref[...].astype(F32)
    own = aux[...]
    high = own.astype(BF16).astype(F32)
    rest = own - high
    mid = rest.astype(BF16).astype(F32)
    low = rest - mid
    sub = lax.broadcasted_iota(jnp.int32, (8, TOK), 0)
    first = jnp.where(sub < HEADS, high, pltpu.roll(mid, HEADS, 0))
    second = jnp.where(sub < HEADS, low, own)
    kvg[sp, 2 * HEAD_DIM : BLK, :] = jnp.concatenate([first, second], axis=0).astype(BF16)

    lane = lax.broadcasted_iota(jnp.int32, (TOK, TOK), 1)
    for pair in range(HEADS // 2):
        both = q_ref[:, pair * TOK : (pair + 1) * TOK].astype(F32) * (HEAD_DIM**-0.5)
        for half in range(2):
            turned = both if half == 0 else pltpu.roll(both, HEAD_DIM, 1)
            qs[pl.ds((pair * 2 + half) * TOK, TOK), :] = jnp.where(lane < HEAD_DIM, turned, 0.0).astype(BF16)
    query_doc = jnp.broadcast_to(own[HEADS : HEADS + 1, :], (TOK, TOK)).T
    top[...] = jnp.full_like(top, very_low)
    acc[...] = jnp.zeros_like(acc)

    with jax.named_scope("barrier"):
        pl.semaphore_wait(barrier, experts - 1 + NT - 1)

    def plane_at(g):
        return (z + ORDER[g] + NZ) % NZ

    def prepare():
        in_copies["ids"].wait()
        in_copies["weights"].wait()
        turn[...] = jnp.zeros_like(turn)
        turn[0:2, 0:ROWS] = ids_ref[...].astype(F32)
        turn[2:4, 0:ROWS] = weights_ref[...]
        along = turn[0:8, 0:ROWS]
        columns = turn[...].T[0:ROWS, :]
        low = lax.broadcasted_iota(jnp.int32, (ROWS, ROWS), 0)
        high = lax.broadcasted_iota(jnp.int32, (ROWS, ROWS), 1)
        lane = lax.broadcasted_iota(jnp.int32, (ROWS, 2 * WIDE), 1)
        spread = jnp.where(
            lax.broadcasted_iota(jnp.int32, (ROWS, WIDE), 1) % ROWS == lax.broadcasted_iota(jnp.int32, (ROWS, WIDE), 0),
            1.0, 0.0,
        ).astype(BF16)
        piece_of = (lax.broadcasted_iota(jnp.int32, (8, WIDE), 1) // ROWS).astype(F32)
        targets = []
        for k in range(2):
            line, column = along[k : k + 1, :], columns[:, k : k + 1]
            rank_line = jnp.zeros((1, ROWS), F32)
            rank_column = jnp.zeros((ROWS, 1), F32)
            for other in range(2):
                same = (columns[:, other : other + 1] == line) & (low < high)
                rank_line = rank_line + jnp.sum(jnp.where(same, 1.0, 0.0), axis=0, keepdims=True)
                same = (along[other : other + 1, :] == column) & (high < low)
                rank_column = rank_column + jnp.sum(jnp.where(same, 1.0, 0.0), axis=1, keepdims=True)
            slot = jnp.broadcast_to(line * 2.0 + rank_line, (8, ROWS)).astype(BF16)
            targets.append(jnp.dot(slot, spread, preferred_element_type=F32) * PIECES + piece_of)
            base = (column * 2.0 + rank_column) * PIECES
            for piece in range(PIECES):
                want = (base + piece).astype(jnp.int32)
                for plane in range(NZ):
                    spots = lax.broadcasted_iota(jnp.int32, (ROWS, TOK), 1) + plane * TOK
                    rows = slice((k * PIECES + piece) * ROWS, (k * PIECES + piece + 1) * ROWS)
                    pick[plane, rows, :] = jnp.where(spots == want, 1.0, 0.0).astype(BF16)
        spots = lax.broadcasted_iota(jnp.int32, (experts * 16, WIDE), 0)
        hit = (spots == targets[0][0:1, :].astype(jnp.int32)) | (spots == targets[1][0:1, :].astype(jnp.int32))
        chosen[...] = jnp.where(hit, 1.0, 0.0).astype(BF16)
        src = lax.broadcasted_iota(jnp.int32, (TOK, TOK), 0)
        dst = lax.broadcasted_iota(jnp.int32, (TOK, TOK), 1)
        choose[0] = jnp.where((dst // 8 == src % 16) & (dst % 8 == src // 16), 1.0, 0.0).astype(BF16)
        choose[1] = jnp.where((src // 8 == dst % 16) & (src % 8 == dst // 16), 1.0, 0.0).astype(BF16)

    def push(slot, target):
        remote(kvg.at[slot], kvg.at[slot], send, recv.at[slot], target, tp).start()

    def arrived(slot):
        remote(kvg.at[slot], kvg.at[slot], send, recv.at[slot], sp, (tp + 1) % NT).wait_recv()

    def spread(slot):
        push(slot, index_of(z, x + 1, c))
        push(slot, index_of(z, x + 3, c))
        push(slot, index_of(z, x + 2, c))
        push(slot, index_of(z, x, c + 1))

    def across(back):
        for step in (1, 3, 2):
            slot = index_of(z - back, x + step, c)
            arrived(slot)
            push(slot, index_of(z, x, c + 1))

    def beside(back):
        for step in range(NX):
            arrived(index_of(z - back, x + step, c + 1))

    extra = index_of(z - 5, x + 3, c + 1)
    extra_off = jnp.where((x == 0) & (c == 0) & (z >= 5), 0.0, -64.0)

    def attend(back):
        plane = (z - back + NZ) % NZ
        slots = [plane * PLANE + k for k in range(PLANE)]
        off = jnp.where(z >= back, 0.0, -64.0)
        offs = [off] * PLANE
        if back == BACK:
            slots.append(extra)
            offs.append(extra_off)
        width = len(slots) * TOK
        gate_first = own[:, 0:1]
        row8 = lax.broadcasted_iota(jnp.int32, (8, TOK), 0)
        blocks = []
        for k, (slot, shift) in enumerate(zip(slots, offs)):
            parts = kvg[slot, 2 * HEAD_DIM : BLK, :].astype(F32)
            upper, lower = parts[0:8], parts[8:16]
            gates = gate_first - (upper + pltpu.roll(upper, HEADS, 0) + lower)
            bias[:, k * TOK : (k + 1) * TOK] = jnp.where(row8 < HEADS, gates, lower + shift)
            blocks.append(kvg[slot, 0 : 2 * HEAD_DIM, :])
        kv = jnp.concatenate(blocks, axis=1)
        row = lax.broadcasted_iota(jnp.int32, kv.shape, 0)
        turned_v[0:width, :] = jnp.where(row < HEAD_DIM, jnp.ones_like(kv), kv).T
        allowed = jnp.concatenate([query_doc] * len(slots), axis=1) == bias[HEADS : HEADS + 1, 0:width]
        if back == 0:
            key_pos = lax.broadcasted_iota(jnp.int32, (TOK, width), 1)
            query_pos = lax.broadcasted_iota(jnp.int32, (TOK, width), 0) + (x * NC + c) * TOK
            allowed = allowed & (key_pos <= query_pos)
        for head in range(HEADS):
            rows = slice(head * TOK, (head + 1) * TOK)
            scores = jnp.dot(qs[rows, :], kv, preferred_element_type=F32)
            scores = jnp.where(allowed, scores + bias[head : head + 1, 0:width], very_low)
            top_old = top[rows, :]
            top_new = jnp.maximum(top_old, jnp.max(scores, axis=1, keepdims=True))
            soft[rows, 0:width] = jnp.exp(scores - top_new[:, 0:1]).astype(BF16)
            acc[rows, :] = acc[rows, :] * jnp.exp(top_old - top_new)
            top[rows, :] = top_new
        acc[...] += jnp.dot(soft[:, 0:width], turned_v[0:width, :], preferred_element_type=F32)

    one, two, three, four = (index_of(z - back, x, c) for back in (1, 2, 3, 4))
    push(sp, index_of(z + 1, x, c))
    push(sp, index_of(z + 2, x, c))
    spread(sp)
    push(sp, index_of(z + 5, x + 1, c + 1))

    @pl.when(c == 0)
    def _():
        share_down()

    with jax.named_scope("prepare"):
        prepare()
    with jax.named_scope("w_one"):
        arrived(one)
    spread(one)
    with jax.named_scope("w_two"):
        arrived(two)
    push(two, index_of(z + 1, x, c))
    push(two, index_of(z + 2, x, c))
    spread(two)
    with jax.named_scope("w_across0"):
        across(0)
    with jax.named_scope("w_beside0"):
        beside(0)
    with jax.named_scope("attend0"):
        attend(0)
    with jax.named_scope("w_across1"):
        across(1)
    with jax.named_scope("w_three"):
        arrived(three)
    spread(three)
    with jax.named_scope("w_beside1"):
        beside(1)
    with jax.named_scope("attend1"):
        attend(1)
    with jax.named_scope("w_four"):
        arrived(four)
    spread(four)

    @pl.when(c == 0)
    def _():
        with jax.named_scope("pass_down"):
            pass_down()

    with jax.named_scope("w_across2"):
        across(2)
    with jax.named_scope("w_across3"):
        across(3)
    with jax.named_scope("w_beside2"):
        beside(2)
    with jax.named_scope("attend2"):
        attend(2)

    with jax.named_scope("w_across4"):
        across(4)
    with jax.named_scope("w_beside3"):
        beside(3)
    with jax.named_scope("attend3"):
        attend(3)
    with jax.named_scope("w_beside4"):
        beside(4)
    with jax.named_scope("w_extra"):
        arrived(extra)
    with jax.named_scope("attend4"):
        attend(4)

    with jax.named_scope("project"):
        done = []
        for head in range(HEADS):
            summed = acc[head * TOK : (head + 1) * TOK, :]
            done.append(summed / pltpu.roll(summed, HEAD_DIM, 1))
        for pair in range(HEADS // 2):
            moved = pltpu.roll(done[2 * pair], HEAD_DIM, 1)
            att[:, pair * TOK : (pair + 1) * TOK] = jnp.where(lane < HEAD_DIM, moved, done[2 * pair + 1]).astype(BF16)
        for step in (1, 3, 2):
            other = (tp + step) % NT
            remote(
                att.at[pl.ds(pl.multiple_of(other * ROWS, ROWS), ROWS)], planes.at[tp], asend, arecv.at[tp], sp, other
            ).start()
        load.wait()
        in_copies["res"].wait()
        in_copies["gain"].wait()
        depth = HEADS * HEAD_DIM

        def part_of(rows, group):
            weights = proj[pl.ds(pl.multiple_of(group * depth, depth), depth), :]
            return jnp.dot(rows, weights, preferred_element_type=F32)

        total = part_of(att[pl.ds(pl.multiple_of(tp * ROWS, ROWS), ROWS), :], tp)
        for step in (1, 3, 2):
            other = (tp + step) % NT
            remote(planes.at[other], planes.at[other], asend, arecv.at[other], sp, other).wait_recv()
            total = total + part_of(planes[other], other)
        stream = (res_ref[...].astype(F32) + total).astype(BF16)
        kept[...] = stream
        stream = stream.astype(F32)
        normed = stream * lax.rsqrt(jnp.mean(stream * stream, axis=1, keepdims=True) + norm_eps)
        normed = (normed * gain_ref[...]).astype(BF16)
        for piece in range(PIECES):
            stacked[piece * ROWS : (piece + 1) * ROWS, :] = normed[:, piece * WIDE : (piece + 1) * WIDE]

    for g in range(NZ):
        plane = (z - ORDER[g] + NZ) % NZ
        rows = pl.ds(pl.multiple_of(plane * TOK, TOK), TOK)
        picked = jnp.dot(chosen[rows, :], stacked[...], preferred_element_type=F32).astype(BF16)
        sent[pl.ds(pl.multiple_of(plane * PLANE, PLANE), PLANE)] = picked.reshape(PLANE, 16, WIDE)

        def one_row(k, carry, plane=plane):
            target = plane * PLANE + k
            remote(sent.at[target], came.at[tp, sp], dsend, drecv.at[z], target, tp).start()
            return carry

        if ORDER[g] == 0:
            for step in range(1, PLANE):
                target = plane * PLANE + (x * NC + c + step) % PLANE
                remote(sent.at[target], came.at[tp, sp], dsend, drecv.at[z], target, tp).start()
            pltpu.make_async_copy(sent.at[sp], came.at[tp, sp], drecv.at[z]).start()
        else:
            lax.fori_loop(0, PLANE, one_row, 0)

    def group(ref, source, plane, half=None):
        if half is None:
            return ref.at[source, pl.ds(pl.multiple_of(plane * PLANE, PLANE), PLANE)]
        return ref.at[source, pl.ds(pl.multiple_of(plane * PLANE + half * (PLANE // 2), PLANE // 2), PLANE // 2)]

    def share(g):
        plane = plane_at(g)
        ref = group(came, tp, plane)
        remote(ref, ref, dsend, drecv.at[plane], sp, right).wait_recv()
        remote(ref, ref, ysend, yl.at[g], sp, right).start()
        remote(ref, ref, ysend, yr.at[g], sp, left).start()

    def relay(g):
        plane = plane_at(g)
        ref = group(came, left, plane)
        remote(ref, ref, ysend, yl.at[g], sp, right).wait_recv()
        ref = group(came, left, plane, 0)
        remote(ref, ref, ysend, ya.at[g], sp, right).start()
        ref = group(came, right, plane)
        remote(ref, ref, ysend, yr.at[g], sp, left).wait_recv()
        ref = group(came, right, plane, 1)
        remote(ref, ref, ysend, yb.at[g], sp, left).start()

    def gathered(g):
        plane = plane_at(g)
        ref = group(came, far, plane, 0)
        remote(ref, ref, ysend, ya.at[g], sp, right).wait_recv()
        ref = group(came, far, plane, 1)
        remote(ref, ref, ysend, yb.at[g], sp, right).wait_recv()

    def compute(chunk):
        for k in range(2):
            plane = plane_at(2 * chunk + k)
            for source in range(NT):
                rows = came[source, pl.ds(pl.multiple_of(plane * PLANE, PLANE), PLANE)].reshape(TOK, WIDE)
                ordered = jnp.dot(choose[0], rows, preferred_element_type=F32).astype(BF16)
                q = (k * NT + source) * 16
                for piece in range(PIECES):
                    xrows[q : q + 16, piece * WIDE : (piece + 1) * WIDE] = ordered[piece * 16 : piece * 16 + 16, :]
        rows = xrows[...]
        gate = jnp.dot(rows, w_gate[...], preferred_element_type=F32)
        upper = jnp.dot(rows, w_up[...], preferred_element_type=F32)
        hidden[...] = (gate / (1.0 + jnp.exp(-gate)) * upper).astype(BF16)

    def multiply(chunk):
        part = jnp.dot(hidden[...], w_down[tp], preferred_element_type=F32).astype(BF16)
        for k in range(2):
            for source in range(NT):
                q = (k * NT + source) * 16
                pieces[2 * chunk + k, source] = part[q : q + 16, :]

    def send_hidden(chunk):
        for k in range(2):
            g = 2 * chunk + k
            for source in range(NT):
                q = (k * NT + source) * 16
                hid_out[g, source] = hidden[q : q + 16, :]
            hid_in[g, tp] = hid_out[g, tp]
            for other in (right, left, far):
                remote(hid_out.at[g, other], hid_in.at[g, tp], hsend, hrecv.at[g], sp, other).start()

    def finish(chunk):
        for k in range(2):
            g = 2 * chunk + k
            some = hid_in.at[g, pl.ds(0, NT - 1)]
            remote(some, some, hsend, hrecv.at[g], sp, right).wait_recv()
        total = jnp.zeros((32, D), F32)
        for source in range(NT):
            rows = hid_in[2 * chunk : 2 * chunk + 2, source].reshape(32, WIDE)
            total = total + jnp.dot(rows, w_down[source], preferred_element_type=F32)
        total = total.astype(BF16)
        for k in range(2):
            hand_back(2 * chunk + k, total[16 * k : 16 * k + 16, :])

    half = D // 2

    def first_halves(g):
        remote(pieces.at[g, far, :, pl.ds(0, half)], half_l.at[g], rsend, ra.at[g], sp, right).start()
        remote(pieces.at[g, far, :, pl.ds(half, half)], half_r.at[g], rsend, rb.at[g], sp, left).start()

    def add_half(g):
        remote(half_l.at[g], half_l.at[g], rsend, ra.at[g], sp, right).wait_recv()
        mine = pieces[g, right]
        to_r[g, :, 0:half] = (mine[:, 0:half].astype(F32) + half_l[g].astype(F32)).astype(BF16)
        to_r[g, :, half:] = mine[:, half:]
        remote(to_r.at[g], full_l.at[g], rsend, rl.at[g], sp, right).start()
        remote(half_r.at[g], half_r.at[g], rsend, rb.at[g], sp, right).wait_recv()
        mine = pieces[g, left]
        to_l[g, :, half:] = (mine[:, half:].astype(F32) + half_r[g].astype(F32)).astype(BF16)
        to_l[g, :, 0:half] = mine[:, 0:half]
        remote(to_l.at[g], full_r.at[g], rsend, rr.at[g], sp, left).start()

    def give_back(g):
        plane = plane_at(g)
        remote(full_l.at[g], full_l.at[g], rsend, rl.at[g], sp, right).wait_recv()
        remote(full_r.at[g], full_r.at[g], rsend, rr.at[g], sp, right).wait_recv()
        total = pieces[g, tp].astype(F32) + full_l[g].astype(F32) + full_r[g].astype(F32)
        hand_back(g, total.astype(BF16))

    def hand_back(g, total):
        plane = plane_at(g)
        stacked = jnp.concatenate([total[:, k * WIDE : (k + 1) * WIDE] for k in range(PIECES)], axis=0)
        mixed = jnp.dot(choose[1], stacked, preferred_element_type=F32).astype(BF16)
        back[pl.ds(pl.multiple_of(g * PLANE, PLANE), PLANE)] = mixed.reshape(PLANE, 16, WIDE)

        def one_row(k, carry):
            target = plane * PLANE + k
            remote(back.at[g * PLANE + k], final.at[sp], fsend, frecv.at[z], target, tp).start()
            return carry

        if ORDER[g] == 0:
            own = x * NC + c
            for step in range(1, PLANE):
                k = (own + step) % PLANE
                remote(
                    back.at[g * PLANE + k], final.at[sp], fsend, frecv.at[z], plane * PLANE + k, tp
                ).start()
            pltpu.make_async_copy(back.at[g * PLANE + own], final.at[sp], frecv.at[z]).start()
        else:
            lax.fori_loop(0, PLANE, one_row, 0)

    chunks = NZ // 2
    for g in range(AHEAD):
        with jax.named_scope(f"share{g}"):
            share(g)
    for g in range(AHEAD, NZ):
        with jax.named_scope(f"relay{g - AHEAD}"):
            relay(g - AHEAD)
        with jax.named_scope(f"share{g}"):
            share(g)
    for load_w in loads[1:]:
        load_w.wait()

    @pl.when(c == 1)
    def _():
        loads[0].wait()


    def first_return(chunk):
        @pl.when(c == 1)
        def _():
            for g in (2 * chunk, 2 * chunk + 1):
                with jax.named_scope(f"add_half{g}"):
                    add_half(g)

    def last_return(chunk):
        @pl.when(c == 0)
        def _():
            if chunk == 0:
                with jax.named_scope("all_down"):
                    all_down()
            with jax.named_scope(f"finish{chunk}"):
                finish(chunk)

        @pl.when(c == 1)
        def _():
            for g in (2 * chunk, 2 * chunk + 1):
                with jax.named_scope(f"back{g}"):
                    give_back(g)

    for chunk in range(chunks):
        for g in (2 * chunk, 2 * chunk + 1):
            with jax.named_scope(f"gathered{g}"):
                gathered(g)
        with jax.named_scope(f"compute{chunk}"):
            compute(chunk)

        @pl.when(c == 0)
        def _(chunk=chunk):
            send_hidden(chunk)

        @pl.when(c == 1)
        def _(chunk=chunk):
            with jax.named_scope(f"multiply{chunk}"):
                multiply(chunk)
            first_halves(2 * chunk)
            first_halves(2 * chunk + 1)

        if chunk < 2:
            for g in (2 * chunk + AHEAD, 2 * chunk + AHEAD + 1):
                with jax.named_scope(f"relay{g}"):
                    relay(g)
        if chunk > 0:
            first_return(chunk - 1)
        if chunk > 1:
            last_return(chunk - 2)
    last_return(chunks - 2)
    first_return(chunks - 1)
    last_return(chunks - 1)

    total = jnp.zeros((2 * PIECES * ROWS, WIDE), F32)
    for g in range(NZ):
        plane = (z - ORDER[g] + NZ) % NZ
        ref = final.at[pl.ds(pl.multiple_of(plane * PLANE, PLANE), PLANE)]
        with jax.named_scope(f"take{g}"):
            remote(ref, ref, fsend, frecv.at[plane], sp, right).wait_recv()
        rows = final[pl.ds(pl.multiple_of(plane * PLANE, PLANE), PLANE)].reshape(TOK, WIDE)
        total = total + jnp.dot(pick[plane], rows, preferred_element_type=F32)
    columns = turn[...].T[0:ROWS, :]
    weight0, weight1 = columns[:, 2:3], columns[:, 3:4]
    for piece in range(PIECES):
        lanes = slice(piece * WIDE, (piece + 1) * WIDE)
        one = total[piece * ROWS : (piece + 1) * ROWS]
        two = total[(PIECES + piece) * ROWS : (PIECES + piece + 1) * ROWS]
        out_ref[:, lanes] = (kept[:, lanes].astype(F32) + (weight0 * one + weight1 * two)).astype(BF16)

    some = sent.at[pl.ds(0, experts - 1)]
    remote(some, some, dsend, drecv.at[0], sp, right).wait_send()
    some = came.at[pl.ds(0, 3)]
    remote(some, some, ysend, yl.at[0], sp, right).wait_send()

    @pl.when(c == 0)
    def _():
        some = w_down.at[pl.ds(0, 3)]
        remote(some, some, gsend, gl.at[0], sp, right).wait_send()
        some = hid_in.at[pl.ds(0, 6)]
        remote(some, some, hsend, hrecv.at[0], sp, right).wait_send()

    @pl.when(c == 1)
    def _():
        some = pieces.at[pl.ds(0, 6)]
        remote(some, some, rsend, ra.at[0], sp, right).wait_send()

    some = final.at[pl.ds(0, experts - 1)]
    remote(some, some, fsend, frecv.at[0], sp, right).wait_send()

    count = 5 + 15 + 20
    remote(kvg.at[pl.ds(0, count)], kvg.at[pl.ds(0, count)], send, recv.at[0], sp, (tp + 1) % NT).wait_send()
    remote(planes.at[pl.ds(0, 3)], planes.at[pl.ds(0, 3)], asend, arecv.at[0], sp, (tp + 1) % NT).wait_send()


def local(
    queries, keys, values, cum_gate, doc_ids, residual, out_proj, norm_gain, route_ids, route_weights,
    expert_gate, expert_up, expert_down,
):
    anywhere = pl.BlockSpec(memory_space=pl.ANY)
    dma, experts = pltpu.SemaphoreType.DMA, NZ * PLANE
    wide_heads = HEADS * HEAD_DIM
    return pl.pallas_call(
        layer_kernel,
        out_shape=jax.ShapeDtypeStruct((ROWS, D), BF16),
        in_specs=[anywhere] * 13,
        out_specs=pl.BlockSpec(memory_space=pltpu.VMEM),
        scratch_shapes=[
            pltpu.VMEM((TOK, wide_heads), BF16),
            pltpu.VMEM((HEADS, TOK), F32),
            pltpu.VMEM((1, TOK), jnp.int32),
            pltpu.VMEM((ROWS, D), BF16),
            pltpu.VMEM((1, D), F32),
            pltpu.VMEM((2, ROWS), jnp.int32),
            pltpu.VMEM((2, ROWS), F32),
            pltpu.VMEM((experts, BLK, TOK), BF16),
            pltpu.VMEM((8, TOK), F32),
            pltpu.VMEM((HEADS * TOK, TOK), BF16),
            pltpu.VMEM((8, (PLANE + 1) * TOK), F32),
            pltpu.VMEM((HEADS * TOK, TOK), F32),
            pltpu.VMEM((HEADS * TOK, TOK), F32),
            pltpu.VMEM((HEADS * TOK, (PLANE + 1) * TOK), BF16),
            pltpu.VMEM(((PLANE + 1) * TOK, TOK), BF16),
            pltpu.VMEM((TOK, wide_heads), BF16),
            pltpu.VMEM((NT, ROWS, wide_heads), BF16),
            pltpu.VMEM((NT * wide_heads, D), BF16),
            pltpu.VMEM((ROWS, D), BF16),
            pltpu.VMEM((PIECES * ROWS, WIDE), BF16),
            pltpu.VMEM((TOK, TOK), F32),
            pltpu.VMEM((experts * 16, WIDE), BF16),
            pltpu.VMEM((2, TOK, TOK), BF16),
            pltpu.VMEM((experts, 16, WIDE), BF16),
            pltpu.VMEM((NT, experts, 16, WIDE), BF16),
            pltpu.VMEM((NZ, 2 * PIECES * ROWS, TOK), BF16),
            pltpu.VMEM((TOK, D), BF16),
            pltpu.VMEM((D, WIDE), BF16),
            pltpu.VMEM((D, WIDE), BF16),
            pltpu.VMEM((NT, WIDE, D), BF16),
            pltpu.VMEM((TOK, WIDE), BF16),
            pltpu.VMEM((NZ, NT, 16, WIDE), BF16),
            pltpu.VMEM((NZ, NT, 16, WIDE), BF16),
            pltpu.VMEM((NZ, NT, 16, D), BF16),
            pltpu.VMEM((NZ, 16, D // 2), BF16),
            pltpu.VMEM((NZ, 16, D // 2), BF16),
            pltpu.VMEM((NZ, 16, D), BF16),
            pltpu.VMEM((NZ, 16, D), BF16),
            pltpu.VMEM((NZ, 16, D), BF16),
            pltpu.VMEM((NZ, 16, D), BF16),
            pltpu.VMEM((experts, 16, WIDE), BF16),
            pltpu.VMEM((experts, 16, WIDE), BF16),
            dma((9,)), dma((experts,)), dma, dma((NT,)), dma, dma,
            dma((3,)), dma, dma((NZ,)), dma, dma((NZ,)), dma((NZ,)), dma((NZ,)), dma((NZ,)),
            dma, dma((NZ,)), dma((NZ,)), dma((NZ,)), dma((NZ,)), dma, dma((NZ,)),
            dma, dma((3,)), dma((3,)), dma, dma((NZ,)),
        ],
        compiler_params=pltpu.CompilerParams(
            collective_id=0, has_side_effects=True, vmem_limit_bytes=60 << 20
        ),
        name="layer",
    )(
        queries, keys.T, values.T, cum_gate.T, doc_ids[None], residual, norm_gain[None], out_proj,
        route_ids.T, route_weights.T, expert_gate, expert_up, expert_down,
    )


def solution(mesh):
    in_specs = (
        P("sp", "tp"),
        P("sp", "tp"),
        P("sp", "tp"),
        P("sp", "tp"),
        P("sp"),
        P(("sp", "tp"), None),
        P(),
        P(),
        P(("sp", "tp"), None),
        P(("sp", "tp"), None),
        P("sp", None, "tp"),
        P("sp", None, "tp"),
        P("sp", "tp", None),
    )
    out_specs = P(("sp", "tp"), None)
    return jax.shard_map(local, mesh=mesh, in_specs=in_specs, out_specs=out_specs, check_vma=False)
```

```python
import functools

import jax
import jax.numpy as jnp
from jax import lax
from jax.experimental import pallas as pl
from jax.experimental.pallas import tpu as pltpu
from jax.sharding import PartitionSpec as P

MESH = pl.DeviceIdType.MESH
F32, BF16 = jnp.float32, jnp.bfloat16

D = 2048
HEAD_DIM = 64
NZ, NX, NC, NT = 8, 4, 2, 4
PLANE = NX * NC
TOK = 128
HEADS = 4
ROWS = 32
BLK = 144
BACK = 4
WIDE = 256
PIECES = D // WIDE
ORDER = (0, 1, 4, -3, 3, -2, 2, -1)
very_low = -1e30
norm_eps = 1e-06


def at(sp, tp):
    return {"sp": sp, "tp": tp}


def remote(src, dst, send, recv, sp, tp):
    return pltpu.make_async_remote_copy(
        src_ref=src, dst_ref=dst, send_sem=send, recv_sem=recv, device_id=at(sp, tp), device_id_type=MESH
    )


def index_of(z, x, c):
    return ((z + NZ) % NZ * NX + (x + NX) % NX) * NC + (c + NC) % NC


def place():
    sp, tp = lax.axis_index("sp"), lax.axis_index("tp")
    return sp, tp, sp // PLANE, sp // NC % NX, sp % NC


def layer_kernel(
    q_hbm, k_hbm, v_hbm, gates_hbm, doc_hbm, res_hbm, gain_hbm, proj_hbm,
    ids_hbm, weights_hbm, gate_hbm, up_hbm, down_hbm,
    out_ref,
    q_ref, gates_ref, doc_ref, res_ref, gain_ref, ids_ref, weights_ref,
    kvg, aux, qs, bias, top, acc, soft, turned_v, att, planes, proj, kept, stacked,
    turn, chosen, choose, sent, came, pick, xrows, w_gate, w_up, w_down,
    hidden, hid_out, hid_in, pieces, half_l, half_r, full_l, full_r, to_r, to_l, back, final,
    insem, recv, send, arecv, asend, psem,
    wsem, dsend, drecv, ysend, yl, yr, ya, yb, rsend, ra, rb, rl, rr, fsend, frecv,
    gsend, gl, gr, hsend, hrecv,
):
    sp, tp, z, x, c = place()
    right, left, far = (tp + 1) % NT, (tp + 3) % NT, (tp + 2) % NT
    experts = NZ * PLANE
    barrier = pltpu.get_barrier_semaphore()
    in_copies = {}
    for k, (name, hbm, vmem) in enumerate((
        ("k", k_hbm, kvg.at[sp, pl.ds(0, HEAD_DIM)]), ("v", v_hbm, kvg.at[sp, pl.ds(HEAD_DIM, HEAD_DIM)]),
        ("gates", gates_hbm, gates_ref), ("doc", doc_hbm, doc_ref), ("q", q_hbm, q_ref), ("ids", ids_hbm, ids_ref),
        ("weights", weights_hbm, weights_ref), ("res", res_hbm, res_ref), ("gain", gain_hbm, gain_ref),
    )):
        in_copies[name] = pltpu.make_async_copy(hbm, vmem, insem.at[k])
        in_copies[name].start()

    def greet(step, carry):
        pl.semaphore_signal(barrier, inc=1, device_id=at((sp + step) % experts, tp), device_id_type=MESH)
        return carry

    lax.fori_loop(1, experts, greet, 0)
    for step in range(1, NT):
        pl.semaphore_signal(barrier, inc=1, device_id=at(sp, (tp + step) % NT), device_id_type=MESH)
    load = pltpu.make_async_copy(proj_hbm, proj, psem)
    load.start()
    loads = [
        pltpu.make_async_copy(hbm.at[0], vmem, wsem.at[k])
        for k, (hbm, vmem) in enumerate(((down_hbm, w_down.at[tp]), (gate_hbm, w_gate), (up_hbm, w_up)))
    ]
    for load_w in loads:
        load_w.start()
    for name in ("k", "v", "gates", "doc", "q"):
        in_copies[name].wait()

    def part_down(source, part):
        return w_down.at[source, pl.ds(part * (WIDE // 2), WIDE // 2)]

    def share_down():
        loads[0].wait()
        for part in (0, 1):
            ref = part_down(tp, part)
            remote(ref, ref, gsend, gl.at[part], sp, right).start()
            ref = part_down(tp, 1 - part)
            remote(ref, ref, gsend, gr.at[1 - part], sp, left).start()

    def pass_down():
        ref = part_down(left, 0)
        remote(ref, ref, gsend, gl.at[0], sp, right).wait_recv()
        remote(ref, ref, gsend, gl.at[2], sp, right).start()
        ref = part_down(right, 1)
        remote(ref, ref, gsend, gr.at[1], sp, right).wait_recv()
        remote(ref, ref, gsend, gr.at[2], sp, left).start()

    def all_down():
        for source, part, sem in ((left, 1, gl.at[1]), (right, 0, gr.at[0]), (far, 0, gl.at[2]), (far, 1, gr.at[2])):
            ref = part_down(source, part)
            remote(ref, ref, gsend, sem, sp, right).wait_recv()

    aux[...] = jnp.zeros_like(aux)
    aux[0:HEADS, :] = gates_ref[...]
    aux[HEADS : HEADS + 1, :] = doc_ref[...].astype(F32)
    own = aux[...]
    high = own.astype(BF16).astype(F32)
    rest = own - high
    mid = rest.astype(BF16).astype(F32)
    low = rest - mid
    sub = lax.broadcasted_iota(jnp.int32, (8, TOK), 0)
    first = jnp.where(sub < HEADS, high, pltpu.roll(mid, HEADS, 0))
    second = jnp.where(sub < HEADS, low, own)
    kvg[sp, 2 * HEAD_DIM : BLK, :] = jnp.concatenate([first, second], axis=0).astype(BF16)

    lane = lax.broadcasted_iota(jnp.int32, (TOK, TOK), 1)
    for pair in range(HEADS // 2):
        both = q_ref[:, pair * TOK : (pair + 1) * TOK].astype(F32) * (HEAD_DIM**-0.5)
        for half in range(2):
            turned = both if half == 0 else pltpu.roll(both, HEAD_DIM, 1)
            qs[pl.ds((pair * 2 + half) * TOK, TOK), :] = jnp.where(lane < HEAD_DIM, turned, 0.0).astype(BF16)
    query_doc = jnp.broadcast_to(own[HEADS : HEADS + 1, :], (TOK, TOK)).T
    top[...] = jnp.full_like(top, very_low)
    acc[...] = jnp.zeros_like(acc)

    with jax.named_scope("barrier"):
        pl.semaphore_wait(barrier, experts - 1 + NT - 1)

    def plane_at(g):
        return (z + ORDER[g] + NZ) % NZ

    def prepare():
        in_copies["ids"].wait()
        in_copies["weights"].wait()
        turn[...] = jnp.zeros_like(turn)
        turn[0:2, 0:ROWS] = ids_ref[...].astype(F32)
        turn[2:4, 0:ROWS] = weights_ref[...]
        along = turn[0:8, 0:ROWS]
        columns = turn[...].T[0:ROWS, :]
        low = lax.broadcasted_iota(jnp.int32, (ROWS, ROWS), 0)
        high = lax.broadcasted_iota(jnp.int32, (ROWS, ROWS), 1)
        lane = lax.broadcasted_iota(jnp.int32, (ROWS, 2 * WIDE), 1)
        spread = jnp.where(
            lax.broadcasted_iota(jnp.int32, (ROWS, WIDE), 1) % ROWS == lax.broadcasted_iota(jnp.int32, (ROWS, WIDE), 0),
            1.0, 0.0,
        ).astype(BF16)
        piece_of = (lax.broadcasted_iota(jnp.int32, (8, WIDE), 1) // ROWS).astype(F32)
        targets = []
        for k in range(2):
            line, column = along[k : k + 1, :], columns[:, k : k + 1]
            rank_line = jnp.zeros((1, ROWS), F32)
            rank_column = jnp.zeros((ROWS, 1), F32)
            for other in range(2):
                same = (columns[:, other : other + 1] == line) & (low < high)
                rank_line = rank_line + jnp.sum(jnp.where(same, 1.0, 0.0), axis=0, keepdims=True)
                same = (along[other : other + 1, :] == column) & (high < low)
                rank_column = rank_column + jnp.sum(jnp.where(same, 1.0, 0.0), axis=1, keepdims=True)
            slot = jnp.broadcast_to(line * 2.0 + rank_line, (8, ROWS)).astype(BF16)
            targets.append(jnp.dot(slot, spread, preferred_element_type=F32) * PIECES + piece_of)
            base = (column * 2.0 + rank_column) * PIECES
            for piece in range(PIECES):
                want = (base + piece).astype(jnp.int32)
                for plane in range(NZ):
                    spots = lax.broadcasted_iota(jnp.int32, (ROWS, TOK), 1) + plane * TOK
                    rows = slice((k * PIECES + piece) * ROWS, (k * PIECES + piece + 1) * ROWS)
                    pick[plane, rows, :] = jnp.where(spots == want, 1.0, 0.0).astype(BF16)
        spots = lax.broadcasted_iota(jnp.int32, (experts * 16, WIDE), 0)
        hit = (spots == targets[0][0:1, :].astype(jnp.int32)) | (spots == targets[1][0:1, :].astype(jnp.int32))
        chosen[...] = jnp.where(hit, 1.0, 0.0).astype(BF16)
        src = lax.broadcasted_iota(jnp.int32, (TOK, TOK), 0)
        dst = lax.broadcasted_iota(jnp.int32, (TOK, TOK), 1)
        choose[0] = jnp.where((dst // 8 == src % 16) & (dst % 8 == src // 16), 1.0, 0.0).astype(BF16)
        choose[1] = jnp.where((src // 8 == dst % 16) & (src % 8 == dst // 16), 1.0, 0.0).astype(BF16)

    def push(slot, target):
        remote(kvg.at[slot], kvg.at[slot], send, recv.at[slot], target, tp).start()

    def arrived(slot):
        remote(kvg.at[slot], kvg.at[slot], send, recv.at[slot], sp, (tp + 1) % NT).wait_recv()

    def spread(slot):
        push(slot, index_of(z, x + 1, c))
        push(slot, index_of(z, x + 3, c))
        push(slot, index_of(z, x + 2, c))
        push(slot, index_of(z, x, c + 1))

    def across(back):
        for step in (1, 3, 2):
            slot = index_of(z - back, x + step, c)
            arrived(slot)
            push(slot, index_of(z, x, c + 1))

    def beside(back):
        for step in range(NX):
            arrived(index_of(z - back, x + step, c + 1))

    extra = index_of(z - 5, x + 3, c + 1)
    extra_off = jnp.where((x == 0) & (c == 0) & (z >= 5), 0.0, -64.0)

    def attend(back):
        plane = (z - back + NZ) % NZ
        slots = [plane * PLANE + k for k in range(PLANE)]
        off = jnp.where(z >= back, 0.0, -64.0)
        offs = [off] * PLANE
        if back == BACK:
            slots.append(extra)
            offs.append(extra_off)
        width = len(slots) * TOK
        gate_first = own[:, 0:1]
        row8 = lax.broadcasted_iota(jnp.int32, (8, TOK), 0)
        blocks = []
        for k, (slot, shift) in enumerate(zip(slots, offs)):
            parts = kvg[slot, 2 * HEAD_DIM : BLK, :].astype(F32)
            upper, lower = parts[0:8], parts[8:16]
            gates = gate_first - (upper + pltpu.roll(upper, HEADS, 0) + lower)
            bias[:, k * TOK : (k + 1) * TOK] = jnp.where(row8 < HEADS, gates, lower + shift)
            blocks.append(kvg[slot, 0 : 2 * HEAD_DIM, :])
        kv = jnp.concatenate(blocks, axis=1)
        row = lax.broadcasted_iota(jnp.int32, kv.shape, 0)
        turned_v[0:width, :] = jnp.where(row < HEAD_DIM, jnp.ones_like(kv), kv).T
        allowed = jnp.concatenate([query_doc] * len(slots), axis=1) == bias[HEADS : HEADS + 1, 0:width]
        if back == 0:
            key_pos = lax.broadcasted_iota(jnp.int32, (TOK, width), 1)
            query_pos = lax.broadcasted_iota(jnp.int32, (TOK, width), 0) + (x * NC + c) * TOK
            allowed = allowed & (key_pos <= query_pos)
        for head in range(HEADS):
            rows = slice(head * TOK, (head + 1) * TOK)
            scores = jnp.dot(qs[rows, :], kv, preferred_element_type=F32)
            scores = jnp.where(allowed, scores + bias[head : head + 1, 0:width], very_low)
            top_old = top[rows, :]
            top_new = jnp.maximum(top_old, jnp.max(scores, axis=1, keepdims=True))
            soft[rows, 0:width] = jnp.exp(scores - top_new[:, 0:1]).astype(BF16)
            acc[rows, :] = acc[rows, :] * jnp.exp(top_old - top_new)
            top[rows, :] = top_new
        acc[...] += jnp.dot(soft[:, 0:width], turned_v[0:width, :], preferred_element_type=F32)

    one, two, three, four = (index_of(z - back, x, c) for back in (1, 2, 3, 4))
    push(sp, index_of(z + 1, x, c))
    push(sp, index_of(z + 2, x, c))
    spread(sp)
    push(sp, index_of(z + 5, x + 1, c + 1))

    @pl.when(c == 0)
    def _():
        share_down()

    with jax.named_scope("prepare"):
        prepare()
    with jax.named_scope("w_one"):
        arrived(one)
    spread(one)
    with jax.named_scope("w_two"):
        arrived(two)
    push(two, index_of(z + 1, x, c))
    push(two, index_of(z + 2, x, c))
    spread(two)
    with jax.named_scope("w_across0"):
        across(0)
    with jax.named_scope("w_beside0"):
        beside(0)
    with jax.named_scope("attend0"):
        attend(0)
    with jax.named_scope("w_three"):
        arrived(three)
    spread(three)
    with jax.named_scope("w_across1"):
        across(1)
    with jax.named_scope("w_four"):
        arrived(four)
    spread(four)
    with jax.named_scope("w_beside1"):
        beside(1)
    with jax.named_scope("attend1"):
        attend(1)

    with jax.named_scope("w_across2"):
        across(2)
    with jax.named_scope("w_across3"):
        across(3)
    with jax.named_scope("w_beside2"):
        beside(2)
    with jax.named_scope("attend2"):
        attend(2)
    with jax.named_scope("w_across4"):
        across(4)
    with jax.named_scope("w_beside3"):
        beside(3)
    with jax.named_scope("attend3"):
        attend(3)
    with jax.named_scope("w_beside4"):
        beside(4)
    with jax.named_scope("w_extra"):
        arrived(extra)
    with jax.named_scope("attend4"):
        attend(4)

    for load_w in loads[1:]:
        load_w.wait()

    @pl.when(c == 1)
    def _():
        loads[0].wait()


    with jax.named_scope("project"):
        with jax.named_scope("p_heads"):
            done = []
            for head in range(HEADS):
                summed = acc[head * TOK : (head + 1) * TOK, :]
                done.append(summed / pltpu.roll(summed, HEAD_DIM, 1))
            for pair in range(HEADS // 2):
                moved = pltpu.roll(done[2 * pair], HEAD_DIM, 1)
                att[:, pair * TOK : (pair + 1) * TOK] = jnp.where(lane < HEAD_DIM, moved, done[2 * pair + 1]).astype(BF16)
            for step in (1, 3, 2):
                other = (tp + step) % NT
                remote(
                    att.at[pl.ds(pl.multiple_of(other * ROWS, ROWS), ROWS)], planes.at[tp], asend, arecv.at[tp], sp, other
                ).start()

        @pl.when(c == 0)
        def _():
            pass_down()

        load.wait()
        in_copies["res"].wait()
        in_copies["gain"].wait()
        depth = HEADS * HEAD_DIM

        def part_of(rows, group):
            weights = proj[pl.ds(pl.multiple_of(group * depth, depth), depth), :]
            return jnp.dot(rows, weights, preferred_element_type=F32)

        total = part_of(att[pl.ds(pl.multiple_of(tp * ROWS, ROWS), ROWS), :], tp)
        for step in (1, 3, 2):
            other = (tp + step) % NT
            remote(planes.at[other], planes.at[other], asend, arecv.at[other], sp, other).wait_recv()
            total = total + part_of(planes[other], other)
        with jax.named_scope("p_norm"):
            stream = (res_ref[...].astype(F32) + total).astype(BF16)
            kept[...] = stream
            stream = stream.astype(F32)
            normed = stream * lax.rsqrt(jnp.mean(stream * stream, axis=1, keepdims=True) + norm_eps)
            normed = (normed * gain_ref[...]).astype(BF16)
            for piece in range(PIECES):
                stacked[piece * ROWS : (piece + 1) * ROWS, :] = normed[:, piece * WIDE : (piece + 1) * WIDE]

    def dispatch(g):
        plane = (z - ORDER[g] + NZ) % NZ
        rows = pl.ds(pl.multiple_of(plane * TOK, TOK), TOK)
        picked = jnp.dot(chosen[rows, :], stacked[...], preferred_element_type=F32).astype(BF16)
        sent[pl.ds(pl.multiple_of(plane * PLANE, PLANE), PLANE)] = picked.reshape(PLANE, 16, WIDE)

        def one_row(k, carry, plane=plane):
            target = plane * PLANE + k
            remote(sent.at[target], came.at[tp, sp], dsend, drecv.at[z], target, tp).start()
            return carry

        if ORDER[g] == 0:
            for step in range(1, PLANE):
                target = plane * PLANE + (x * NC + c + step) % PLANE
                remote(sent.at[target], came.at[tp, sp], dsend, drecv.at[z], target, tp).start()
            pltpu.make_async_copy(sent.at[sp], came.at[tp, sp], drecv.at[z]).start()
        else:
            lax.fori_loop(0, PLANE, one_row, 0)

    def group(ref, source, plane, half=None):
        if half is None:
            return ref.at[source, pl.ds(pl.multiple_of(plane * PLANE, PLANE), PLANE)]
        return ref.at[source, pl.ds(pl.multiple_of(plane * PLANE + half * (PLANE // 2), PLANE // 2), PLANE // 2)]

    def share(g):
        plane = plane_at(g)
        ref = group(came, tp, plane)
        remote(ref, ref, dsend, drecv.at[plane], sp, right).wait_recv()
        remote(ref, ref, ysend, yl.at[g], sp, right).start()
        remote(ref, ref, ysend, yr.at[g], sp, left).start()

    def relay(g):
        plane = plane_at(g)
        ref = group(came, left, plane)
        remote(ref, ref, ysend, yl.at[g], sp, right).wait_recv()
        ref = group(came, left, plane, 0)
        remote(ref, ref, ysend, ya.at[g], sp, right).start()
        ref = group(came, right, plane)
        remote(ref, ref, ysend, yr.at[g], sp, left).wait_recv()
        ref = group(came, right, plane, 1)
        remote(ref, ref, ysend, yb.at[g], sp, left).start()

    def gathered(g):
        plane = plane_at(g)
        ref = group(came, far, plane, 0)
        remote(ref, ref, ysend, ya.at[g], sp, right).wait_recv()
        ref = group(came, far, plane, 1)
        remote(ref, ref, ysend, yb.at[g], sp, right).wait_recv()

    def compute(chunk):
        for k in range(2):
            plane = plane_at(2 * chunk + k)
            for source in range(NT):
                rows = came[source, pl.ds(pl.multiple_of(plane * PLANE, PLANE), PLANE)].reshape(TOK, WIDE)
                ordered = jnp.dot(choose[0], rows, preferred_element_type=F32).astype(BF16)
                q = (k * NT + source) * 16
                for piece in range(PIECES):
                    xrows[q : q + 16, piece * WIDE : (piece + 1) * WIDE] = ordered[piece * 16 : piece * 16 + 16, :]
        rows = xrows[...]
        gate = jnp.dot(rows, w_gate[...], preferred_element_type=F32)
        upper = jnp.dot(rows, w_up[...], preferred_element_type=F32)
        hidden[...] = (gate / (1.0 + jnp.exp(-gate)) * upper).astype(BF16)

    def multiply(chunk):
        part = jnp.dot(hidden[...], w_down[tp], preferred_element_type=F32).astype(BF16)
        for k in range(2):
            for source in range(NT):
                q = (k * NT + source) * 16
                pieces[2 * chunk + k, source] = part[q : q + 16, :]

    def send_hidden(chunk):
        for k in range(2):
            g = 2 * chunk + k
            for source in range(NT):
                q = (k * NT + source) * 16
                hid_out[g, source] = hidden[q : q + 16, :]
            hid_in[g, tp] = hid_out[g, tp]
            for other in (right, left, far):
                remote(hid_out.at[g, other], hid_in.at[g, tp], hsend, hrecv.at[g], sp, other).start()

    def finish(chunk):
        for k in range(2):
            g = 2 * chunk + k
            some = hid_in.at[g, pl.ds(0, NT - 1)]
            remote(some, some, hsend, hrecv.at[g], sp, right).wait_recv()
        total = jnp.zeros((32, D), F32)
        for source in range(NT):
            rows = hid_in[2 * chunk : 2 * chunk + 2, source].reshape(32, WIDE)
            total = total + jnp.dot(rows, w_down[source], preferred_element_type=F32)
        total = total.astype(BF16)
        for k in range(2):
            hand_back(2 * chunk + k, total[16 * k : 16 * k + 16, :])

    half = D // 2

    def first_halves(g):
        remote(pieces.at[g, far, :, pl.ds(0, half)], half_l.at[g], rsend, ra.at[g], sp, right).start()
        remote(pieces.at[g, far, :, pl.ds(half, half)], half_r.at[g], rsend, rb.at[g], sp, left).start()

    def add_half(g):
        remote(half_l.at[g], half_l.at[g], rsend, ra.at[g], sp, right).wait_recv()
        mine = pieces[g, right]
        to_r[g, :, 0:half] = (mine[:, 0:half].astype(F32) + half_l[g].astype(F32)).astype(BF16)
        to_r[g, :, half:] = mine[:, half:]
        remote(to_r.at[g], full_l.at[g], rsend, rl.at[g], sp, right).start()
        remote(half_r.at[g], half_r.at[g], rsend, rb.at[g], sp, right).wait_recv()
        mine = pieces[g, left]
        to_l[g, :, half:] = (mine[:, half:].astype(F32) + half_r[g].astype(F32)).astype(BF16)
        to_l[g, :, 0:half] = mine[:, 0:half]
        remote(to_l.at[g], full_r.at[g], rsend, rr.at[g], sp, left).start()

    def give_back(g):
        plane = plane_at(g)
        remote(full_l.at[g], full_l.at[g], rsend, rl.at[g], sp, right).wait_recv()
        remote(full_r.at[g], full_r.at[g], rsend, rr.at[g], sp, right).wait_recv()
        total = pieces[g, tp].astype(F32) + full_l[g].astype(F32) + full_r[g].astype(F32)
        hand_back(g, total.astype(BF16))

    def hand_back(g, total):
        plane = plane_at(g)
        stacked = jnp.concatenate([total[:, k * WIDE : (k + 1) * WIDE] for k in range(PIECES)], axis=0)
        mixed = jnp.dot(choose[1], stacked, preferred_element_type=F32).astype(BF16)
        back[pl.ds(pl.multiple_of(g * PLANE, PLANE), PLANE)] = mixed.reshape(PLANE, 16, WIDE)

        def one_row(k, carry):
            target = plane * PLANE + k
            remote(back.at[g * PLANE + k], final.at[sp], fsend, frecv.at[z], target, tp).start()
            return carry

        if ORDER[g] == 0:
            own = x * NC + c
            for step in range(1, PLANE):
                k = (own + step) % PLANE
                remote(
                    back.at[g * PLANE + k], final.at[sp], fsend, frecv.at[z], plane * PLANE + k, tp
                ).start()
            pltpu.make_async_copy(back.at[g * PLANE + own], final.at[sp], frecv.at[z]).start()
        else:
            lax.fori_loop(0, PLANE, one_row, 0)

    chunks = NZ // 2
    def first_return(chunk):
        @pl.when(c == 1)
        def _():
            for g in (2 * chunk, 2 * chunk + 1):
                with jax.named_scope(f"add_half{g}"):
                    add_half(g)

    def last_return(chunk):
        @pl.when(c == 1)
        def _():
            for g in (2 * chunk, 2 * chunk + 1):
                with jax.named_scope(f"back{g}"):
                    give_back(g)

    def from_hidden(chunk):
        @pl.when(c == 0)
        def _():
            if chunk == 0:
                with jax.named_scope("all_down"):
                    all_down()
            with jax.named_scope(f"finish{chunk}"):
                finish(chunk)

    def expert(chunk):
        for g in (2 * chunk, 2 * chunk + 1):
            with jax.named_scope(f"gathered{g}"):
                gathered(g)
        with jax.named_scope(f"compute{chunk}"):
            compute(chunk)

        @pl.when(c == 0)
        def _():
            send_hidden(chunk)

        @pl.when(c == 1)
        def _():
            with jax.named_scope(f"multiply{chunk}"):
                multiply(chunk)
            first_halves(2 * chunk)
            first_halves(2 * chunk + 1)

    D_, S, R, E, H, A, B = dispatch, share, relay, expert, from_hidden, first_return, last_return
    for step, number in (
        (D_, 0), (D_, 1), (D_, 2), (D_, 3), (D_, 4), (S, 0), (D_, 5), (D_, 6), (D_, 7), (S, 1), (R, 0), (S, 2), (S, 3),
        (R, 1), (R, 2), (S, 4), (S, 5), (E, 0), (R, 3), (S, 6), (S, 7), (A, 0), (R, 4), (R, 5), (H, 0), (E, 1),
        (R, 6), (R, 7), (E, 2), (H, 1), (A, 1), (B, 0), (E, 3), (H, 2), (A, 2), (B, 1), (H, 3), (A, 3), (B, 2), (B, 3),
    ):
        with jax.named_scope(f"{step.__name__}{number}"):
            step(number)

    some = sent.at[pl.ds(0, experts - 1)]
    remote(some, some, dsend, drecv.at[0], sp, right).wait_send()
    some = came.at[pl.ds(0, 3)]
    remote(some, some, ysend, yl.at[0], sp, right).wait_send()

    @pl.when(c == 0)
    def _():
        some = w_down.at[pl.ds(0, 3)]
        remote(some, some, gsend, gl.at[0], sp, right).wait_send()
        some = hid_in.at[pl.ds(0, 6)]
        remote(some, some, hsend, hrecv.at[0], sp, right).wait_send()

    @pl.when(c == 1)
    def _():
        some = pieces.at[pl.ds(0, 6)]
        remote(some, some, rsend, ra.at[0], sp, right).wait_send()


    count = 5 + 15 + 20
    remote(kvg.at[pl.ds(0, count)], kvg.at[pl.ds(0, count)], send, recv.at[0], sp, (tp + 1) % NT).wait_send()
    remote(planes.at[pl.ds(0, 3)], planes.at[pl.ds(0, 3)], asend, arecv.at[0], sp, (tp + 1) % NT).wait_send()

    columns = turn[...].T[0:ROWS, :]
    total = jnp.zeros((2 * PIECES * ROWS, WIDE), F32)
    for g in range(NZ):
        plane = (z - ORDER[g] + NZ) % NZ
        ref = final.at[pl.ds(pl.multiple_of(plane * PLANE, PLANE), PLANE)]
        with jax.named_scope(f"take{g}"):
            remote(ref, ref, fsend, frecv.at[plane], sp, right).wait_recv()
        rows = final[pl.ds(pl.multiple_of(plane * PLANE, PLANE), PLANE)].reshape(TOK, WIDE)
        total = total + jnp.dot(pick[plane], rows, preferred_element_type=F32)
    weight0, weight1 = columns[:, 2:3], columns[:, 3:4]
    for piece in range(PIECES):
        lanes = slice(piece * WIDE, (piece + 1) * WIDE)
        one = total[piece * ROWS : (piece + 1) * ROWS]
        two = total[(PIECES + piece) * ROWS : (PIECES + piece + 1) * ROWS]
        out_ref[:, lanes] = (kept[:, lanes].astype(F32) + (weight0 * one + weight1 * two)).astype(BF16)

    some = final.at[pl.ds(0, experts - 1)]
    remote(some, some, fsend, frecv.at[0], sp, right).wait_send()


def local(
    queries, keys, values, cum_gate, doc_ids, residual, out_proj, norm_gain, route_ids, route_weights,
    expert_gate, expert_up, expert_down,
):
    anywhere = pl.BlockSpec(memory_space=pl.ANY)
    dma, experts = pltpu.SemaphoreType.DMA, NZ * PLANE
    wide_heads = HEADS * HEAD_DIM
    return pl.pallas_call(
        layer_kernel,
        out_shape=jax.ShapeDtypeStruct((ROWS, D), BF16),
        in_specs=[anywhere] * 13,
        out_specs=pl.BlockSpec(memory_space=pltpu.VMEM),
        scratch_shapes=[
            pltpu.VMEM((TOK, wide_heads), BF16),
            pltpu.VMEM((HEADS, TOK), F32),
            pltpu.VMEM((1, TOK), jnp.int32),
            pltpu.VMEM((ROWS, D), BF16),
            pltpu.VMEM((1, D), F32),
            pltpu.VMEM((2, ROWS), jnp.int32),
            pltpu.VMEM((2, ROWS), F32),
            pltpu.VMEM((experts, BLK, TOK), BF16),
            pltpu.VMEM((8, TOK), F32),
            pltpu.VMEM((HEADS * TOK, TOK), BF16),
            pltpu.VMEM((8, (PLANE + 1) * TOK), F32),
            pltpu.VMEM((HEADS * TOK, TOK), F32),
            pltpu.VMEM((HEADS * TOK, TOK), F32),
            pltpu.VMEM((HEADS * TOK, (PLANE + 1) * TOK), BF16),
            pltpu.VMEM(((PLANE + 1) * TOK, TOK), BF16),
            pltpu.VMEM((TOK, wide_heads), BF16),
            pltpu.VMEM((NT, ROWS, wide_heads), BF16),
            pltpu.VMEM((NT * wide_heads, D), BF16),
            pltpu.VMEM((ROWS, D), BF16),
            pltpu.VMEM((PIECES * ROWS, WIDE), BF16),
            pltpu.VMEM((TOK, TOK), F32),
            pltpu.VMEM((experts * 16, WIDE), BF16),
            pltpu.VMEM((2, TOK, TOK), BF16),
            pltpu.VMEM((experts, 16, WIDE), BF16),
            pltpu.VMEM((NT, experts, 16, WIDE), BF16),
            pltpu.VMEM((NZ, 2 * PIECES * ROWS, TOK), BF16),
            pltpu.VMEM((TOK, D), BF16),
            pltpu.VMEM((D, WIDE), BF16),
            pltpu.VMEM((D, WIDE), BF16),
            pltpu.VMEM((NT, WIDE, D), BF16),
            pltpu.VMEM((TOK, WIDE), BF16),
            pltpu.VMEM((NZ, NT, 16, WIDE), BF16),
            pltpu.VMEM((NZ, NT, 16, WIDE), BF16),
            pltpu.VMEM((NZ, NT, 16, D), BF16),
            pltpu.VMEM((NZ, 16, D // 2), BF16),
            pltpu.VMEM((NZ, 16, D // 2), BF16),
            pltpu.VMEM((NZ, 16, D), BF16),
            pltpu.VMEM((NZ, 16, D), BF16),
            pltpu.VMEM((NZ, 16, D), BF16),
            pltpu.VMEM((NZ, 16, D), BF16),
            pltpu.VMEM((experts, 16, WIDE), BF16),
            pltpu.VMEM((experts, 16, WIDE), BF16),
            dma((9,)), dma((experts,)), dma, dma((NT,)), dma, dma,
            dma((3,)), dma, dma((NZ,)), dma, dma((NZ,)), dma((NZ,)), dma((NZ,)), dma((NZ,)),
            dma, dma((NZ,)), dma((NZ,)), dma((NZ,)), dma((NZ,)), dma, dma((NZ,)),
            dma, dma((3,)), dma((3,)), dma, dma((NZ,)),
        ],
        compiler_params=pltpu.CompilerParams(
            collective_id=0, has_side_effects=True, vmem_limit_bytes=60 << 20
        ),
        name="layer",
    )(
        queries, keys.T, values.T, cum_gate.T, doc_ids[None], residual, norm_gain[None], out_proj,
        route_ids.T, route_weights.T, expert_gate, expert_up, expert_down,
    )


def solution(mesh):
    in_specs = (
        P("sp", "tp"),
        P("sp", "tp"),
        P("sp", "tp"),
        P("sp", "tp"),
        P("sp"),
        P(("sp", "tp"), None),
        P(),
        P(),
        P(("sp", "tp"), None),
        P(("sp", "tp"), None),
        P("sp", None, "tp"),
        P("sp", None, "tp"),
        P("sp", "tp", None),
    )
    out_specs = P(("sp", "tp"), None)
    return jax.shard_map(local, mesh=mesh, in_specs=in_specs, out_specs=out_specs, check_vma=False)
```

```python
import functools

import jax
import jax.numpy as jnp
from jax import lax
from jax.experimental import pallas as pl
from jax.experimental.pallas import tpu as pltpu
from jax.sharding import PartitionSpec as P

MESH = pl.DeviceIdType.MESH
F32, BF16 = jnp.float32, jnp.bfloat16

D = 2048
HEAD_DIM = 64
NZ, NX, NC, NT = 8, 4, 2, 4
PLANE = NX * NC
TOK = 128
HEADS = 4
ROWS = 32
BLK = 144
BACK = 4
WIDE = 256
PIECES = D // WIDE
ORDER = (0, 1, 4, -3, 3, -2, 2, -1)
PAIRS = ((0, 2), (3, 4), (5, 6), (1, 7))
very_low = -1e30
norm_eps = 1e-06


def at(sp, tp):
    return {"sp": sp, "tp": tp}


def remote(src, dst, send, recv, sp, tp):
    return pltpu.make_async_remote_copy(
        src_ref=src, dst_ref=dst, send_sem=send, recv_sem=recv, device_id=at(sp, tp), device_id_type=MESH
    )


def index_of(z, x, c):
    return ((z + NZ) % NZ * NX + (x + NX) % NX) * NC + (c + NC) % NC


def place():
    sp, tp = lax.axis_index("sp"), lax.axis_index("tp")
    return sp, tp, sp // PLANE, sp // NC % NX, sp % NC


def layer_kernel(
    q_hbm, k_hbm, v_hbm, gates_hbm, doc_hbm, res_hbm, gain_hbm, proj_hbm,
    ids_hbm, weights_hbm, gate_hbm, up_hbm, down_hbm,
    out_ref,
    q_ref, gates_ref, doc_ref, res_ref, gain_ref, ids_ref, weights_ref,
    kvg, aux, qs, bias, top, acc, soft, turned_v, att, planes, proj, kept, stacked,
    turn, chosen, choose, sent, came, pick, xrows, w_gate, w_up, w_down,
    hidden, hid_out, hid_in, pieces, half_l, half_r, full_l, full_r, to_r, to_l, back, final, taken,
    insem, recv, send, arecv, asend, psem,
    wsem, dsend, drecv, ysend, yl, yr, ya, yb, rsend, ra, rb, rl, rr, fsend, frecv,
    gsend, gl, gr, hsend, hrecv,
):
    sp, tp, z, x, c = place()
    right, left, far = (tp + 1) % NT, (tp + 3) % NT, (tp + 2) % NT
    experts = NZ * PLANE
    barrier = pltpu.get_barrier_semaphore()
    for step in range(1, NT):
        pl.semaphore_signal(barrier, inc=1, device_id=at(sp, (tp + step) % NT), device_id_type=MESH)

    def greet(turn_of, carry):
        for part in range(7):
            other = (sp + 1 + turn_of * 7 + part) % experts
            pl.semaphore_signal(barrier, inc=1, device_id=at(other, tp), device_id_type=MESH)
        return carry

    lax.fori_loop(0, (experts - 1) // 7, greet, 0)
    in_copies = {}
    for k, (name, hbm, vmem) in enumerate((
        ("k", k_hbm, kvg.at[sp, pl.ds(0, HEAD_DIM)]), ("v", v_hbm, kvg.at[sp, pl.ds(HEAD_DIM, HEAD_DIM)]),
        ("gates", gates_hbm, gates_ref), ("doc", doc_hbm, doc_ref), ("q", q_hbm, q_ref), ("ids", ids_hbm, ids_ref),
        ("weights", weights_hbm, weights_ref), ("res", res_hbm, res_ref), ("gain", gain_hbm, gain_ref),
    )):
        in_copies[name] = pltpu.make_async_copy(hbm, vmem, insem.at[k])
        in_copies[name].start()

    load = pltpu.make_async_copy(proj_hbm, proj, psem)
    load.start()
    loads = [
        pltpu.make_async_copy(hbm.at[0], vmem, wsem.at[k])
        for k, (hbm, vmem) in enumerate(((down_hbm, w_down.at[tp]), (gate_hbm, w_gate), (up_hbm, w_up)))
    ]
    for load_w in loads:
        load_w.start()
    for name in ("k", "v", "gates", "doc", "q"):
        in_copies[name].wait()

    def part_down(source, part):
        return w_down.at[source, pl.ds(part * (WIDE // 2), WIDE // 2)]

    def share_down():
        loads[0].wait()
        for part in (0, 1):
            ref = part_down(tp, part)
            remote(ref, ref, gsend, gl.at[part], sp, right).start()
            ref = part_down(tp, 1 - part)
            remote(ref, ref, gsend, gr.at[1 - part], sp, left).start()

    def pass_down():
        ref = part_down(left, 0)
        remote(ref, ref, gsend, gl.at[0], sp, right).wait_recv()
        remote(ref, ref, gsend, gl.at[2], sp, right).start()
        ref = part_down(right, 1)
        remote(ref, ref, gsend, gr.at[1], sp, right).wait_recv()
        remote(ref, ref, gsend, gr.at[2], sp, left).start()

    def all_down():
        for source, part, sem in ((left, 1, gl.at[1]), (right, 0, gr.at[0]), (far, 0, gl.at[2]), (far, 1, gr.at[2])):
            ref = part_down(source, part)
            remote(ref, ref, gsend, sem, sp, right).wait_recv()

    aux[...] = jnp.zeros_like(aux)
    aux[0:HEADS, :] = gates_ref[...]
    aux[HEADS : HEADS + 1, :] = doc_ref[...].astype(F32)
    own = aux[...]
    high = own.astype(BF16).astype(F32)
    rest = own - high
    mid = rest.astype(BF16).astype(F32)
    low = rest - mid
    sub = lax.broadcasted_iota(jnp.int32, (8, TOK), 0)
    first = jnp.where(sub < HEADS, high, pltpu.roll(mid, HEADS, 0))
    second = jnp.where(sub < HEADS, low, own)
    kvg[sp, 2 * HEAD_DIM : BLK, :] = jnp.concatenate([first, second], axis=0).astype(BF16)

    lane = lax.broadcasted_iota(jnp.int32, (TOK, TOK), 1)
    for pair in range(HEADS // 2):
        both = q_ref[:, pair * TOK : (pair + 1) * TOK].astype(F32) * (HEAD_DIM**-0.5)
        for half in range(2):
            turned = both if half == 0 else pltpu.roll(both, HEAD_DIM, 1)
            qs[pl.ds((pair * 2 + half) * TOK, TOK), :] = jnp.where(lane < HEAD_DIM, turned, 0.0).astype(BF16)
    query_doc = jnp.broadcast_to(own[HEADS : HEADS + 1, :], (TOK, TOK)).T
    top[...] = jnp.full_like(top, very_low)
    acc[...] = jnp.zeros_like(acc)

    with jax.named_scope("barrier"):
        pl.semaphore_wait(barrier, experts - 1 + NT - 1)

    def plane_at(g):
        return (z + ORDER[g] + NZ) % NZ

    def prepare():
        in_copies["ids"].wait()
        in_copies["weights"].wait()
        turn[...] = jnp.zeros_like(turn)
        turn[0:2, 0:ROWS] = ids_ref[...].astype(F32)
        turn[2:4, 0:ROWS] = weights_ref[...]
        along = turn[0:8, 0:ROWS]
        columns = turn[...].T[0:ROWS, :]
        low = lax.broadcasted_iota(jnp.int32, (ROWS, ROWS), 0)
        high = lax.broadcasted_iota(jnp.int32, (ROWS, ROWS), 1)
        lane = lax.broadcasted_iota(jnp.int32, (ROWS, 2 * WIDE), 1)
        spread = jnp.where(
            lax.broadcasted_iota(jnp.int32, (ROWS, WIDE), 1) % ROWS == lax.broadcasted_iota(jnp.int32, (ROWS, WIDE), 0),
            1.0, 0.0,
        ).astype(BF16)
        piece_of = (lax.broadcasted_iota(jnp.int32, (8, WIDE), 1) // ROWS).astype(F32)
        targets = []
        for k in range(2):
            line, column = along[k : k + 1, :], columns[:, k : k + 1]
            rank_line = jnp.zeros((1, ROWS), F32)
            rank_column = jnp.zeros((ROWS, 1), F32)
            for other in range(2):
                same = (columns[:, other : other + 1] == line) & (low < high)
                rank_line = rank_line + jnp.sum(jnp.where(same, 1.0, 0.0), axis=0, keepdims=True)
                same = (along[other : other + 1, :] == column) & (high < low)
                rank_column = rank_column + jnp.sum(jnp.where(same, 1.0, 0.0), axis=1, keepdims=True)
            slot = jnp.broadcast_to(line * 2.0 + rank_line, (8, ROWS)).astype(BF16)
            targets.append(jnp.dot(slot, spread, preferred_element_type=F32) * PIECES + piece_of)
            base = (column * 2.0 + rank_column) * PIECES
            for piece in range(PIECES):
                want = (base + piece).astype(jnp.int32)
                for plane in range(NZ):
                    spots = lax.broadcasted_iota(jnp.int32, (ROWS, TOK), 1) + plane * TOK
                    rows = slice((k * PIECES + piece) * ROWS, (k * PIECES + piece + 1) * ROWS)
                    pick[plane, rows, :] = jnp.where(spots == want, 1.0, 0.0).astype(BF16)
        spots = lax.broadcasted_iota(jnp.int32, (experts * 16, WIDE), 0)
        hit = (spots == targets[0][0:1, :].astype(jnp.int32)) | (spots == targets[1][0:1, :].astype(jnp.int32))
        chosen[...] = jnp.where(hit, 1.0, 0.0).astype(BF16)
        src = lax.broadcasted_iota(jnp.int32, (TOK, TOK), 0)
        dst = lax.broadcasted_iota(jnp.int32, (TOK, TOK), 1)
        choose[0] = jnp.where((dst // 8 == src % 16) & (dst % 8 == src // 16), 1.0, 0.0).astype(BF16)
        choose[1] = jnp.where((src // 8 == dst % 16) & (src % 8 == dst // 16), 1.0, 0.0).astype(BF16)

    def push(slot, target):
        remote(kvg.at[slot], kvg.at[slot], send, recv.at[slot], target, tp).start()

    def arrived(slot):
        remote(kvg.at[slot], kvg.at[slot], send, recv.at[slot], sp, (tp + 1) % NT).wait_recv()

    def spread(slot):
        push(slot, index_of(z, x + 1, c))
        push(slot, index_of(z, x + 3, c))
        push(slot, index_of(z, x + 2, c))
        push(slot, index_of(z, x, c + 1))

    def across(back):
        for step in (1, 3, 2):
            slot = index_of(z - back, x + step, c)
            arrived(slot)
            push(slot, index_of(z, x, c + 1))

    def beside(back):
        for step in range(NX):
            arrived(index_of(z - back, x + step, c + 1))

    extra = index_of(z - 5, x + 3, c + 1)
    extra_off = jnp.where((x == 0) & (c == 0) & (z >= 5), 0.0, -64.0)

    def attend(back):
        plane = (z - back + NZ) % NZ
        slots = [plane * PLANE + k for k in range(PLANE)]
        off = jnp.where(z >= back, 0.0, -64.0)
        offs = [off] * PLANE
        if back == BACK:
            slots.append(extra)
            offs.append(extra_off)
        width = len(slots) * TOK
        gate_first = own[:, 0:1]
        row8 = lax.broadcasted_iota(jnp.int32, (8, TOK), 0)
        blocks = []
        for k, (slot, shift) in enumerate(zip(slots, offs)):
            parts = kvg[slot, 2 * HEAD_DIM : BLK, :].astype(F32)
            upper, lower = parts[0:8], parts[8:16]
            gates = gate_first - (upper + pltpu.roll(upper, HEADS, 0) + lower)
            bias[:, k * TOK : (k + 1) * TOK] = jnp.where(row8 < HEADS, gates, lower + shift)
            blocks.append(kvg[slot, 0 : 2 * HEAD_DIM, :])
        kv = jnp.concatenate(blocks, axis=1)
        row = lax.broadcasted_iota(jnp.int32, kv.shape, 0)
        turned_v[0:width, :] = jnp.where(row < HEAD_DIM, jnp.ones_like(kv), kv).T
        allowed = jnp.concatenate([query_doc] * len(slots), axis=1) == bias[HEADS : HEADS + 1, 0:width]
        if back == 0:
            key_pos = lax.broadcasted_iota(jnp.int32, (TOK, width), 1)
            query_pos = lax.broadcasted_iota(jnp.int32, (TOK, width), 0) + (x * NC + c) * TOK
            allowed = allowed & (key_pos <= query_pos)
        for head in range(HEADS):
            rows = slice(head * TOK, (head + 1) * TOK)
            scores = jnp.dot(qs[rows, :], kv, preferred_element_type=F32)
            scores = jnp.where(allowed, scores + bias[head : head + 1, 0:width], very_low)
            top_old = top[rows, :]
            top_new = jnp.maximum(top_old, jnp.max(scores, axis=1, keepdims=True))
            soft[rows, 0:width] = jnp.exp(scores - top_new[:, 0:1]).astype(BF16)
            acc[rows, :] = acc[rows, :] * jnp.exp(top_old - top_new)
            top[rows, :] = top_new
        acc[...] += jnp.dot(soft[:, 0:width], turned_v[0:width, :], preferred_element_type=F32)

    one, two, three, four = (index_of(z - back, x, c) for back in (1, 2, 3, 4))
    push(sp, index_of(z + 1, x, c))
    push(sp, index_of(z + 2, x, c))
    spread(sp)
    push(sp, index_of(z + 5, x + 1, c + 1))

    @pl.when(c == 0)
    def _():
        share_down()

    with jax.named_scope("prepare"):
        prepare()
    with jax.named_scope("w_one"):
        arrived(one)
    spread(one)
    with jax.named_scope("w_two"):
        arrived(two)
    push(two, index_of(z + 1, x, c))
    push(two, index_of(z + 2, x, c))
    spread(two)
    with jax.named_scope("w_across0"):
        across(0)
    with jax.named_scope("w_beside0"):
        beside(0)
    with jax.named_scope("attend0"):
        attend(0)
    with jax.named_scope("w_three"):
        arrived(three)
    spread(three)
    with jax.named_scope("w_across1"):
        across(1)
    with jax.named_scope("w_four"):
        arrived(four)
    spread(four)
    with jax.named_scope("w_beside1"):
        beside(1)
    with jax.named_scope("attend1"):
        attend(1)

    with jax.named_scope("w_across2"):
        across(2)
    with jax.named_scope("w_across3"):
        across(3)
    with jax.named_scope("w_beside2"):
        beside(2)
    with jax.named_scope("attend2"):
        attend(2)
    with jax.named_scope("w_across4"):
        across(4)
    with jax.named_scope("w_beside3"):
        beside(3)
    with jax.named_scope("attend3"):
        attend(3)
    with jax.named_scope("w_beside4"):
        beside(4)
    with jax.named_scope("w_extra"):
        arrived(extra)
    with jax.named_scope("attend4"):
        attend(4)

    for load_w in loads[1:]:
        load_w.wait()

    @pl.when(c == 1)
    def _():
        loads[0].wait()


    with jax.named_scope("project"):
        with jax.named_scope("p_heads"):
            done = []
            for head in range(HEADS):
                summed = acc[head * TOK : (head + 1) * TOK, :]
                done.append(summed / pltpu.roll(summed, HEAD_DIM, 1))
            for pair in range(HEADS // 2):
                moved = pltpu.roll(done[2 * pair], HEAD_DIM, 1)
                att[:, pair * TOK : (pair + 1) * TOK] = jnp.where(lane < HEAD_DIM, moved, done[2 * pair + 1]).astype(BF16)
            for step in (1, 3, 2):
                other = (tp + step) % NT
                remote(
                    att.at[pl.ds(pl.multiple_of(other * ROWS, ROWS), ROWS)], planes.at[tp], asend, arecv.at[tp], sp, other
                ).start()

        @pl.when(c == 0)
        def _():
            pass_down()

        load.wait()
        in_copies["res"].wait()
        in_copies["gain"].wait()
        depth = HEADS * HEAD_DIM

        def part_of(rows, group):
            weights = proj[pl.ds(pl.multiple_of(group * depth, depth), depth), :]
            return jnp.dot(rows, weights, preferred_element_type=F32)

        total = part_of(att[pl.ds(pl.multiple_of(tp * ROWS, ROWS), ROWS), :], tp)
        for step in (1, 3, 2):
            other = (tp + step) % NT
            remote(planes.at[other], planes.at[other], asend, arecv.at[other], sp, other).wait_recv()
            total = total + part_of(planes[other], other)
        with jax.named_scope("p_norm"):
            stream = (res_ref[...].astype(F32) + total).astype(BF16)
            kept[...] = stream
            stream = stream.astype(F32)
            normed = stream * lax.rsqrt(jnp.mean(stream * stream, axis=1, keepdims=True) + norm_eps)
            normed = (normed * gain_ref[...]).astype(BF16)
            for piece in range(PIECES):
                stacked[piece * ROWS : (piece + 1) * ROWS, :] = normed[:, piece * WIDE : (piece + 1) * WIDE]

    def dispatch(g):
        plane = (z - ORDER[g] + NZ) % NZ
        rows = pl.ds(pl.multiple_of(plane * TOK, TOK), TOK)
        picked = jnp.dot(chosen[rows, :], stacked[...], preferred_element_type=F32).astype(BF16)
        sent[pl.ds(pl.multiple_of(plane * PLANE, PLANE), PLANE)] = picked.reshape(PLANE, 16, WIDE)

        def one_row(k, carry, plane=plane):
            target = plane * PLANE + (x * NC + c + k) % PLANE
            remote(sent.at[target], came.at[tp, sp], dsend, drecv.at[z], target, tp).start()
            return carry

        if ORDER[g] == 0:
            for step in range(1, PLANE):
                target = plane * PLANE + (x * NC + c + step) % PLANE
                remote(sent.at[target], came.at[tp, sp], dsend, drecv.at[z], target, tp).start()
            pltpu.make_async_copy(sent.at[sp], came.at[tp, sp], drecv.at[z]).start()
        else:
            lax.fori_loop(0, PLANE, one_row, 0)

    def group(ref, source, plane, half=None):
        if half is None:
            return ref.at[source, pl.ds(pl.multiple_of(plane * PLANE, PLANE), PLANE)]
        return ref.at[source, pl.ds(pl.multiple_of(plane * PLANE + half * (PLANE // 2), PLANE // 2), PLANE // 2)]

    def share(g):
        plane = plane_at(g)
        ref = group(came, tp, plane)
        remote(ref, ref, dsend, drecv.at[plane], sp, right).wait_recv()
        remote(ref, ref, ysend, yl.at[g], sp, right).start()
        remote(ref, ref, ysend, yr.at[g], sp, left).start()

    def relay(g):
        plane = plane_at(g)
        ref = group(came, left, plane)
        remote(ref, ref, ysend, yl.at[g], sp, right).wait_recv()
        ref = group(came, left, plane, 0)
        remote(ref, ref, ysend, ya.at[g], sp, right).start()
        ref = group(came, right, plane)
        remote(ref, ref, ysend, yr.at[g], sp, left).wait_recv()
        ref = group(came, right, plane, 1)
        remote(ref, ref, ysend, yb.at[g], sp, left).start()

    def gathered(g):
        plane = plane_at(g)
        ref = group(came, far, plane, 0)
        remote(ref, ref, ysend, ya.at[g], sp, right).wait_recv()
        ref = group(came, far, plane, 1)
        remote(ref, ref, ysend, yb.at[g], sp, right).wait_recv()

    def compute(chunk):
        for k in range(2):
            plane = plane_at(PAIRS[chunk][k])
            for source in range(NT):
                rows = came[source, pl.ds(pl.multiple_of(plane * PLANE, PLANE), PLANE)].reshape(TOK, WIDE)
                ordered = jnp.dot(choose[0], rows, preferred_element_type=F32).astype(BF16)
                q = (k * NT + source) * 16
                for piece in range(PIECES):
                    xrows[q : q + 16, piece * WIDE : (piece + 1) * WIDE] = ordered[piece * 16 : piece * 16 + 16, :]
        rows = xrows[...]
        gate = jnp.dot(rows, w_gate[...], preferred_element_type=F32)
        upper = jnp.dot(rows, w_up[...], preferred_element_type=F32)
        hidden[...] = (gate / (1.0 + jnp.exp(-gate)) * upper).astype(BF16)

    def multiply(chunk):
        part = jnp.dot(hidden[...], w_down[tp], preferred_element_type=F32).astype(BF16)
        for k in range(2):
            for source in range(NT):
                q = (k * NT + source) * 16
                pieces[PAIRS[chunk][k], source] = part[q : q + 16, :]

    def send_hidden(chunk):
        for k in range(2):
            g = PAIRS[chunk][k]
            for source in range(NT):
                q = (k * NT + source) * 16
                hid_out[g, source] = hidden[q : q + 16, :]
            hid_in[g, tp] = hid_out[g, tp]
            for other in (right, left, far):
                remote(hid_out.at[g, other], hid_in.at[g, tp], hsend, hrecv.at[g], sp, other).start()

    def finish(chunk):
        for k in range(2):
            g = PAIRS[chunk][k]
            some = hid_in.at[g, pl.ds(0, NT - 1)]
            remote(some, some, hsend, hrecv.at[g], sp, right).wait_recv()
        total = jnp.zeros((32, D), F32)
        for source in range(NT):
            rows = jnp.concatenate([hid_in[g, source] for g in PAIRS[chunk]], axis=0)
            total = total + jnp.dot(rows, w_down[source], preferred_element_type=F32)
        total = total.astype(BF16)
        for k in range(2):
            hand_back(PAIRS[chunk][k], total[16 * k : 16 * k + 16, :])

    half = D // 2

    def first_halves(g):
        remote(pieces.at[g, far, :, pl.ds(0, half)], half_l.at[g], rsend, ra.at[g], sp, right).start()
        remote(pieces.at[g, far, :, pl.ds(half, half)], half_r.at[g], rsend, rb.at[g], sp, left).start()

    def add_half(g):
        remote(half_l.at[g], half_l.at[g], rsend, ra.at[g], sp, right).wait_recv()
        mine = pieces[g, right]
        to_r[g, :, 0:half] = (mine[:, 0:half].astype(F32) + half_l[g].astype(F32)).astype(BF16)
        to_r[g, :, half:] = mine[:, half:]
        remote(to_r.at[g], full_l.at[g], rsend, rl.at[g], sp, right).start()
        remote(half_r.at[g], half_r.at[g], rsend, rb.at[g], sp, right).wait_recv()
        mine = pieces[g, left]
        to_l[g, :, half:] = (mine[:, half:].astype(F32) + half_r[g].astype(F32)).astype(BF16)
        to_l[g, :, 0:half] = mine[:, 0:half]
        remote(to_l.at[g], full_r.at[g], rsend, rr.at[g], sp, left).start()

    def give_back(g):
        plane = plane_at(g)
        remote(full_l.at[g], full_l.at[g], rsend, rl.at[g], sp, right).wait_recv()
        remote(full_r.at[g], full_r.at[g], rsend, rr.at[g], sp, right).wait_recv()
        total = pieces[g, tp].astype(F32) + full_l[g].astype(F32) + full_r[g].astype(F32)
        hand_back(g, total.astype(BF16))

    def hand_back(g, total):
        plane = plane_at(g)
        stacked = jnp.concatenate([total[:, k * WIDE : (k + 1) * WIDE] for k in range(PIECES)], axis=0)
        mixed = jnp.dot(choose[1], stacked, preferred_element_type=F32).astype(BF16)
        back[pl.ds(pl.multiple_of(g * PLANE, PLANE), PLANE)] = mixed.reshape(PLANE, 16, WIDE)

        def one_row(k, carry):
            k = (x * NC + c + k) % PLANE
            target = plane * PLANE + k
            remote(back.at[g * PLANE + k], final.at[sp], fsend, frecv.at[z], target, tp).start()
            return carry

        if ORDER[g] == 0:
            own = x * NC + c
            for step in range(1, PLANE):
                k = (own + step) % PLANE
                remote(
                    back.at[g * PLANE + k], final.at[sp], fsend, frecv.at[z], plane * PLANE + k, tp
                ).start()
            pltpu.make_async_copy(back.at[g * PLANE + own], final.at[sp], frecv.at[z]).start()
        else:
            lax.fori_loop(0, PLANE, one_row, 0)

    chunks = NZ // 2
    def first_return(chunk):
        @pl.when(c == 1)
        def _():
            for g in PAIRS[chunk]:
                with jax.named_scope(f"add_half{g}"):
                    add_half(g)

    def last_return(chunk):
        @pl.when(c == 1)
        def _():
            for g in PAIRS[chunk]:
                with jax.named_scope(f"back{g}"):
                    give_back(g)

    def from_hidden(chunk):
        @pl.when(c == 0)
        def _():
            if chunk == 0:
                with jax.named_scope("all_down"):
                    all_down()
            with jax.named_scope(f"finish{chunk}"):
                finish(chunk)

    def expert(chunk):
        for g in PAIRS[chunk]:
            with jax.named_scope(f"gathered{g}"):
                gathered(g)
        with jax.named_scope(f"compute{chunk}"):
            compute(chunk)

        @pl.when(c == 0)
        def _():
            send_hidden(chunk)

        @pl.when(c == 1)
        def _():
            with jax.named_scope(f"multiply{chunk}"):
                multiply(chunk)
            for g in PAIRS[chunk]:
                first_halves(g)

    D_, S, R, E, H, A, B = dispatch, share, relay, expert, from_hidden, first_return, last_return
    for step, number in (
        (D_, 0), (D_, 1), (D_, 2), (D_, 3), (D_, 4), (S, 0), (D_, 5), (D_, 6), (D_, 7), (S, 1), (R, 0), (S, 2), (S, 3),
        (R, 1), (R, 2), (S, 4), (S, 5), (S, 6), (S, 7), (R, 3), (E, 0), (R, 4), (R, 5), (R, 6), (R, 7), (A, 0), (E, 1),
        (E, 2), (H, 0), (A, 1), (B, 0), (E, 3), (H, 1), (A, 2), (B, 1), (H, 2), (A, 3), (B, 2), (H, 3), (B, 3),
    ):
        with jax.named_scope(f"{step.__name__}{number}"):
            step(number)

    some = sent.at[pl.ds(0, experts - 1)]
    remote(some, some, dsend, drecv.at[0], sp, right).wait_send()
    some = came.at[pl.ds(0, 3)]
    remote(some, some, ysend, yl.at[0], sp, right).wait_send()

    @pl.when(c == 0)
    def _():
        some = w_down.at[pl.ds(0, 3)]
        remote(some, some, gsend, gl.at[0], sp, right).wait_send()
        some = hid_in.at[pl.ds(0, 6)]
        remote(some, some, hsend, hrecv.at[0], sp, right).wait_send()

    @pl.when(c == 1)
    def _():
        some = pieces.at[pl.ds(0, 6)]
        remote(some, some, rsend, ra.at[0], sp, right).wait_send()


    count = 5 + 15 + 20
    remote(kvg.at[pl.ds(0, count)], kvg.at[pl.ds(0, count)], send, recv.at[0], sp, (tp + 1) % NT).wait_send()
    remote(planes.at[pl.ds(0, 3)], planes.at[pl.ds(0, 3)], asend, arecv.at[0], sp, (tp + 1) % NT).wait_send()

    columns = turn[...].T[0:ROWS, :]
    for first, g in enumerate(g for pair in PAIRS for g in pair):
        plane = (z - ORDER[g] + NZ) % NZ
        ref = final.at[pl.ds(pl.multiple_of(plane * PLANE, PLANE), PLANE)]
        with jax.named_scope(f"take{g}"):
            remote(ref, ref, fsend, frecv.at[plane], sp, right).wait_recv()
        rows = final[pl.ds(pl.multiple_of(plane * PLANE, PLANE), PLANE)].reshape(TOK, WIDE)
        part = jnp.dot(pick[plane], rows, preferred_element_type=F32)
        taken[...] = part if first == 0 else taken[...] + part
    weight0, weight1 = columns[:, 2:3], columns[:, 3:4]
    for piece in range(PIECES):
        lanes = slice(piece * WIDE, (piece + 1) * WIDE)
        one = taken[piece * ROWS : (piece + 1) * ROWS, :]
        two = taken[(PIECES + piece) * ROWS : (PIECES + piece + 1) * ROWS, :]
        out_ref[:, lanes] = (kept[:, lanes].astype(F32) + (weight0 * one + weight1 * two)).astype(BF16)

    some = final.at[pl.ds(0, experts - 1)]
    remote(some, some, fsend, frecv.at[0], sp, right).wait_send()


def local(
    queries, keys, values, cum_gate, doc_ids, residual, out_proj, norm_gain, route_ids, route_weights,
    expert_gate, expert_up, expert_down,
):
    anywhere = pl.BlockSpec(memory_space=pl.ANY)
    dma, experts = pltpu.SemaphoreType.DMA, NZ * PLANE
    wide_heads = HEADS * HEAD_DIM
    return pl.pallas_call(
        layer_kernel,
        out_shape=pltpu.VMEM((ROWS, D), BF16),
        in_specs=[anywhere] * 13,
        out_specs=pl.BlockSpec(memory_space=pltpu.VMEM),
        scratch_shapes=[
            pltpu.VMEM((TOK, wide_heads), BF16),
            pltpu.VMEM((HEADS, TOK), F32),
            pltpu.VMEM((1, TOK), jnp.int32),
            pltpu.VMEM((ROWS, D), BF16),
            pltpu.VMEM((1, D), F32),
            pltpu.VMEM((2, ROWS), jnp.int32),
            pltpu.VMEM((2, ROWS), F32),
            pltpu.VMEM((experts, BLK, TOK), BF16),
            pltpu.VMEM((8, TOK), F32),
            pltpu.VMEM((HEADS * TOK, TOK), BF16),
            pltpu.VMEM((8, (PLANE + 1) * TOK), F32),
            pltpu.VMEM((HEADS * TOK, TOK), F32),
            pltpu.VMEM((HEADS * TOK, TOK), F32),
            pltpu.VMEM((HEADS * TOK, (PLANE + 1) * TOK), BF16),
            pltpu.VMEM(((PLANE + 1) * TOK, TOK), BF16),
            pltpu.VMEM((TOK, wide_heads), BF16),
            pltpu.VMEM((NT, ROWS, wide_heads), BF16),
            pltpu.VMEM((NT * wide_heads, D), BF16),
            pltpu.VMEM((ROWS, D), BF16),
            pltpu.VMEM((PIECES * ROWS, WIDE), BF16),
            pltpu.VMEM((TOK, TOK), F32),
            pltpu.VMEM((experts * 16, WIDE), BF16),
            pltpu.VMEM((2, TOK, TOK), BF16),
            pltpu.VMEM((experts, 16, WIDE), BF16),
            pltpu.VMEM((NT, experts, 16, WIDE), BF16),
            pltpu.VMEM((NZ, 2 * PIECES * ROWS, TOK), BF16),
            pltpu.VMEM((TOK, D), BF16),
            pltpu.VMEM((D, WIDE), BF16),
            pltpu.VMEM((D, WIDE), BF16),
            pltpu.VMEM((NT, WIDE, D), BF16),
            pltpu.VMEM((TOK, WIDE), BF16),
            pltpu.VMEM((NZ, NT, 16, WIDE), BF16),
            pltpu.VMEM((NZ, NT, 16, WIDE), BF16),
            pltpu.VMEM((NZ, NT, 16, D), BF16),
            pltpu.VMEM((NZ, 16, D // 2), BF16),
            pltpu.VMEM((NZ, 16, D // 2), BF16),
            pltpu.VMEM((NZ, 16, D), BF16),
            pltpu.VMEM((NZ, 16, D), BF16),
            pltpu.VMEM((NZ, 16, D), BF16),
            pltpu.VMEM((NZ, 16, D), BF16),
            pltpu.VMEM((experts, 16, WIDE), BF16),
            pltpu.VMEM((experts, 16, WIDE), BF16),
            pltpu.VMEM((2 * PIECES * ROWS, WIDE), F32),
            dma((9,)), dma((experts,)), dma, dma((NT,)), dma, dma,
            dma((3,)), dma, dma((NZ,)), dma, dma((NZ,)), dma((NZ,)), dma((NZ,)), dma((NZ,)),
            dma, dma((NZ,)), dma((NZ,)), dma((NZ,)), dma((NZ,)), dma, dma((NZ,)),
            dma, dma((3,)), dma((3,)), dma, dma((NZ,)),
        ],
        compiler_params=pltpu.CompilerParams(
            collective_id=0, has_side_effects=True, vmem_limit_bytes=60 << 20
        ),
        name="layer",
    )(
        queries, keys.T, values.T, cum_gate.T, doc_ids[None], residual, norm_gain[None], out_proj,
        route_ids.T, route_weights.T, expert_gate, expert_up, expert_down,
    )


def solution(mesh):
    in_specs = (
        P("sp", "tp"),
        P("sp", "tp"),
        P("sp", "tp"),
        P("sp", "tp"),
        P("sp"),
        P(("sp", "tp"), None),
        P(),
        P(),
        P(("sp", "tp"), None),
        P(("sp", "tp"), None),
        P("sp", None, "tp"),
        P("sp", None, "tp"),
        P("sp", "tp", None),
    )
    out_specs = P(("sp", "tp"), None)
    return jax.shard_map(local, mesh=mesh, in_specs=in_specs, out_specs=out_specs, check_vma=False)
```

```python
import functools

import jax
import jax.numpy as jnp
from jax import lax
from jax.experimental import pallas as pl
from jax.experimental.pallas import tpu as pltpu
from jax.sharding import PartitionSpec as P

MESH = pl.DeviceIdType.MESH
F32, BF16 = jnp.float32, jnp.bfloat16

D = 2048
HEAD_DIM = 64
NZ, NX, NC, NT = 8, 4, 2, 4
PLANE = NX * NC
TOK = 128
HEADS = 4
ROWS = 32
BLK = 144
BACK = 4
WIDE = 256
PIECES = D // WIDE
ORDER = (0, 1, 4, -3, 3, -2, 2, -1)
PAIRS = ((0, 2), (3, 4), (5, 6), (1, 7))
very_low = -1e30
norm_eps = 1e-06


def at(sp, tp):
    return {"sp": sp, "tp": tp}


def remote(src, dst, send, recv, sp, tp):
    return pltpu.make_async_remote_copy(
        src_ref=src, dst_ref=dst, send_sem=send, recv_sem=recv, device_id=at(sp, tp), device_id_type=MESH
    )


def index_of(z, x, c):
    return ((z + NZ) % NZ * NX + (x + NX) % NX) * NC + (c + NC) % NC


def place():
    sp, tp = lax.axis_index("sp"), lax.axis_index("tp")
    return sp, tp, sp // PLANE, sp // NC % NX, sp % NC


def layer_kernel(
    q_hbm, k_hbm, v_hbm, gates_hbm, doc_hbm, res_hbm, gain_hbm, proj_hbm,
    ids_hbm, weights_hbm, gate_hbm, up_hbm, down_hbm,
    out_ref,
    q_ref, gates_ref, doc_ref, res_ref, gain_ref, ids_ref, weights_ref,
    kvg, aux, qs, bias, top, acc, soft, turned_v, att, planes, proj, kept, stacked,
    turn, chosen, choose, sent, came, pick, xrows, w_gate, w_up, w_down,
    hidden, hid_out, hid_in, pieces, half_l, half_r, full_l, full_r, to_r, to_l, back, final, taken,
    insem, recv, send, arecv, asend, psem,
    wsem, dsend, drecv, ysend, yl, yr, ya, yb, rsend, ra, rb, rl, rr, fsend, frecv,
    gsend, gl, gr, hsend, hrecv,
):
    sp, tp, z, x, c = place()
    right, left, far = (tp + 1) % NT, (tp + 3) % NT, (tp + 2) % NT
    experts = NZ * PLANE
    barrier = pltpu.get_barrier_semaphore()
    for step in range(1, NT):
        pl.semaphore_signal(barrier, inc=1, device_id=at(sp, (tp + step) % NT), device_id_type=MESH)

    def greet(turn_of, carry):
        for part in range(7):
            other = (sp + 1 + turn_of * 7 + part) % experts
            pl.semaphore_signal(barrier, inc=1, device_id=at(other, tp), device_id_type=MESH)
        return carry

    lax.fori_loop(0, (experts - 1) // 7, greet, 0)
    in_copies = {}
    for k, (name, hbm, vmem) in enumerate((
        ("k", k_hbm, kvg.at[sp, pl.ds(0, HEAD_DIM)]), ("v", v_hbm, kvg.at[sp, pl.ds(HEAD_DIM, HEAD_DIM)]),
        ("gates", gates_hbm, gates_ref), ("doc", doc_hbm, doc_ref), ("q", q_hbm, q_ref), ("ids", ids_hbm, ids_ref),
        ("weights", weights_hbm, weights_ref), ("res", res_hbm, res_ref), ("gain", gain_hbm, gain_ref),
    )):
        in_copies[name] = pltpu.make_async_copy(hbm, vmem, insem.at[k])
        in_copies[name].start()

    load = pltpu.make_async_copy(proj_hbm, proj, psem)
    load.start()
    loads = [
        pltpu.make_async_copy(hbm.at[0], vmem, wsem.at[k])
        for k, (hbm, vmem) in enumerate(((down_hbm, w_down.at[tp]), (gate_hbm, w_gate), (up_hbm, w_up)))
    ]
    for load_w in loads:
        load_w.start()
    for name in ("k", "v", "gates", "doc", "q"):
        in_copies[name].wait()

    def part_down(source, part):
        return w_down.at[source, pl.ds(part * (WIDE // 2), WIDE // 2)]

    def share_down():
        loads[0].wait()
        for part in (0, 1):
            ref = part_down(tp, part)
            remote(ref, ref, gsend, gl.at[part], sp, right).start()
            ref = part_down(tp, 1 - part)
            remote(ref, ref, gsend, gr.at[1 - part], sp, left).start()

    def pass_down():
        ref = part_down(left, 0)
        remote(ref, ref, gsend, gl.at[0], sp, right).wait_recv()
        remote(ref, ref, gsend, gl.at[2], sp, right).start()
        ref = part_down(right, 1)
        remote(ref, ref, gsend, gr.at[1], sp, right).wait_recv()
        remote(ref, ref, gsend, gr.at[2], sp, left).start()

    def all_down():
        for source, part, sem in ((left, 1, gl.at[1]), (right, 0, gr.at[0]), (far, 0, gl.at[2]), (far, 1, gr.at[2])):
            ref = part_down(source, part)
            remote(ref, ref, gsend, sem, sp, right).wait_recv()

    aux[...] = jnp.zeros_like(aux)
    aux[0:HEADS, :] = gates_ref[...]
    aux[HEADS : HEADS + 1, :] = doc_ref[...].astype(F32)
    own = aux[...]
    high = own.astype(BF16).astype(F32)
    rest = own - high
    mid = rest.astype(BF16).astype(F32)
    low = rest - mid
    sub = lax.broadcasted_iota(jnp.int32, (8, TOK), 0)
    first = jnp.where(sub < HEADS, high, pltpu.roll(mid, HEADS, 0))
    second = jnp.where(sub < HEADS, low, own)
    kvg[sp, 2 * HEAD_DIM : BLK, :] = jnp.concatenate([first, second], axis=0).astype(BF16)

    lane = lax.broadcasted_iota(jnp.int32, (TOK, TOK), 1)
    for pair in range(HEADS // 2):
        both = q_ref[:, pair * TOK : (pair + 1) * TOK].astype(F32) * (HEAD_DIM**-0.5)
        for half in range(2):
            turned = both if half == 0 else pltpu.roll(both, HEAD_DIM, 1)
            qs[pl.ds((pair * 2 + half) * TOK, TOK), :] = jnp.where(lane < HEAD_DIM, turned, 0.0).astype(BF16)
    query_doc = jnp.broadcast_to(own[HEADS : HEADS + 1, :], (TOK, TOK)).T
    top[...] = jnp.full_like(top, very_low)
    acc[...] = jnp.zeros_like(acc)

    with jax.named_scope("barrier"):
        pl.semaphore_wait(barrier, experts - 1 + NT - 1)

    def plane_at(g):
        return (z + ORDER[g] + NZ) % NZ

    def prepare():
        in_copies["ids"].wait()
        in_copies["weights"].wait()
        turn[...] = jnp.zeros_like(turn)
        turn[0:2, 0:ROWS] = ids_ref[...].astype(F32)
        turn[2:4, 0:ROWS] = weights_ref[...]
        along = turn[0:8, 0:ROWS]
        columns = turn[...].T[0:ROWS, :]
        low = lax.broadcasted_iota(jnp.int32, (ROWS, ROWS), 0)
        high = lax.broadcasted_iota(jnp.int32, (ROWS, ROWS), 1)
        lane = lax.broadcasted_iota(jnp.int32, (ROWS, 2 * WIDE), 1)
        spread = jnp.where(
            lax.broadcasted_iota(jnp.int32, (ROWS, WIDE), 1) % ROWS == lax.broadcasted_iota(jnp.int32, (ROWS, WIDE), 0),
            1.0, 0.0,
        ).astype(BF16)
        piece_of = (lax.broadcasted_iota(jnp.int32, (8, WIDE), 1) // ROWS).astype(F32)
        targets = []
        for k in range(2):
            line, column = along[k : k + 1, :], columns[:, k : k + 1]
            rank_line = jnp.zeros((1, ROWS), F32)
            rank_column = jnp.zeros((ROWS, 1), F32)
            for other in range(2):
                same = (columns[:, other : other + 1] == line) & (low < high)
                rank_line = rank_line + jnp.sum(jnp.where(same, 1.0, 0.0), axis=0, keepdims=True)
                same = (along[other : other + 1, :] == column) & (high < low)
                rank_column = rank_column + jnp.sum(jnp.where(same, 1.0, 0.0), axis=1, keepdims=True)
            slot = jnp.broadcast_to(line * 2.0 + rank_line, (8, ROWS)).astype(BF16)
            targets.append(jnp.dot(slot, spread, preferred_element_type=F32) * PIECES + piece_of)
            base = (column * 2.0 + rank_column) * PIECES
            for piece in range(PIECES):
                want = (base + piece).astype(jnp.int32)
                for plane in range(NZ):
                    spots = lax.broadcasted_iota(jnp.int32, (ROWS, TOK), 1) + plane * TOK
                    rows = slice((k * PIECES + piece) * ROWS, (k * PIECES + piece + 1) * ROWS)
                    pick[plane, rows, :] = jnp.where(spots == want, 1.0, 0.0).astype(BF16)
        spots = lax.broadcasted_iota(jnp.int32, (experts * 16, WIDE), 0)
        hit = (spots == targets[0][0:1, :].astype(jnp.int32)) | (spots == targets[1][0:1, :].astype(jnp.int32))
        chosen[...] = jnp.where(hit, 1.0, 0.0).astype(BF16)
        src = lax.broadcasted_iota(jnp.int32, (TOK, TOK), 0)
        dst = lax.broadcasted_iota(jnp.int32, (TOK, TOK), 1)
        choose[0] = jnp.where((dst // 8 == src % 16) & (dst % 8 == src // 16), 1.0, 0.0).astype(BF16)
        choose[1] = jnp.where((src // 8 == dst % 16) & (src % 8 == dst // 16), 1.0, 0.0).astype(BF16)

    def push(slot, target):
        remote(kvg.at[slot], kvg.at[slot], send, recv.at[slot], target, tp).start()

    def arrived(slot):
        remote(kvg.at[slot], kvg.at[slot], send, recv.at[slot], sp, (tp + 1) % NT).wait_recv()

    def spread(slot):
        push(slot, index_of(z, x + 1, c))
        push(slot, index_of(z, x + 3, c))
        push(slot, index_of(z, x + 2, c))
        push(slot, index_of(z, x, c + 1))

    def across(back):
        for step in (1, 3, 2):
            slot = index_of(z - back, x + step, c)
            arrived(slot)
            push(slot, index_of(z, x, c + 1))

    def beside(back):
        for step in range(NX):
            arrived(index_of(z - back, x + step, c + 1))

    extra = index_of(z - 5, x + 3, c + 1)
    extra_off = jnp.where((x == 0) & (c == 0) & (z >= 5), 0.0, -64.0)

    def attend(back):
        plane = (z - back + NZ) % NZ
        slots = [plane * PLANE + k for k in range(PLANE)]
        off = jnp.where(z >= back, 0.0, -64.0)
        offs = [off] * PLANE
        if back == BACK:
            slots.append(extra)
            offs.append(extra_off)
        width = len(slots) * TOK
        gate_first = own[:, 0:1]
        row8 = lax.broadcasted_iota(jnp.int32, (8, TOK), 0)
        blocks = []
        for k, (slot, shift) in enumerate(zip(slots, offs)):
            parts = kvg[slot, 2 * HEAD_DIM : BLK, :].astype(F32)
            upper, lower = parts[0:8], parts[8:16]
            gates = gate_first - (upper + pltpu.roll(upper, HEADS, 0) + lower)
            bias[:, k * TOK : (k + 1) * TOK] = jnp.where(row8 < HEADS, gates, lower + shift)
            blocks.append(kvg[slot, 0 : 2 * HEAD_DIM, :])
        kv = jnp.concatenate(blocks, axis=1)
        row = lax.broadcasted_iota(jnp.int32, kv.shape, 0)
        turned_v[0:width, :] = jnp.where(row < HEAD_DIM, jnp.ones_like(kv), kv).T
        allowed = jnp.concatenate([query_doc] * len(slots), axis=1) == bias[HEADS : HEADS + 1, 0:width]
        if back == 0:
            key_pos = lax.broadcasted_iota(jnp.int32, (TOK, width), 1)
            query_pos = lax.broadcasted_iota(jnp.int32, (TOK, width), 0) + (x * NC + c) * TOK
            allowed = allowed & (key_pos <= query_pos)
        for head in range(HEADS):
            rows = slice(head * TOK, (head + 1) * TOK)
            scores = jnp.dot(qs[rows, :], kv, preferred_element_type=F32)
            scores = jnp.where(allowed, scores + bias[head : head + 1, 0:width], very_low)
            top_old = top[rows, :]
            top_new = jnp.maximum(top_old, jnp.max(scores, axis=1, keepdims=True))
            soft[rows, 0:width] = jnp.exp(scores - top_new[:, 0:1]).astype(BF16)
            acc[rows, :] = acc[rows, :] * jnp.exp(top_old - top_new)
            top[rows, :] = top_new
        acc[...] += jnp.dot(soft[:, 0:width], turned_v[0:width, :], preferred_element_type=F32)

    one, two, three, four = (index_of(z - back, x, c) for back in (1, 2, 3, 4))
    push(sp, index_of(z + 1, x, c))
    push(sp, index_of(z + 2, x, c))
    spread(sp)
    push(sp, index_of(z + 5, x + 1, c + 1))

    @pl.when(c == 0)
    def _():
        share_down()

    with jax.named_scope("prepare"):
        prepare()
    with jax.named_scope("w_one"):
        arrived(one)
    spread(one)
    with jax.named_scope("w_two"):
        arrived(two)
    push(two, index_of(z + 1, x, c))
    push(two, index_of(z + 2, x, c))
    spread(two)
    with jax.named_scope("w_across0"):
        across(0)
    with jax.named_scope("w_beside0"):
        beside(0)
    with jax.named_scope("attend0"):
        attend(0)
    with jax.named_scope("w_three"):
        arrived(three)
    spread(three)
    with jax.named_scope("w_across1"):
        across(1)
    with jax.named_scope("w_four"):
        arrived(four)
    spread(four)
    with jax.named_scope("w_beside1"):
        beside(1)
    with jax.named_scope("attend1"):
        attend(1)

    with jax.named_scope("w_across2"):
        across(2)
    with jax.named_scope("w_across3"):
        across(3)
    with jax.named_scope("w_beside2"):
        beside(2)
    with jax.named_scope("attend2"):
        attend(2)
    with jax.named_scope("w_across4"):
        across(4)
    with jax.named_scope("w_beside3"):
        beside(3)
    with jax.named_scope("attend3"):
        attend(3)
    with jax.named_scope("w_beside4"):
        beside(4)
    with jax.named_scope("w_extra"):
        arrived(extra)
    with jax.named_scope("attend4"):
        attend(4)

    for load_w in loads[1:]:
        load_w.wait()

    @pl.when(c == 1)
    def _():
        loads[0].wait()


    with jax.named_scope("project"):
        with jax.named_scope("p_heads"):
            done = []
            for head in range(HEADS):
                summed = acc[head * TOK : (head + 1) * TOK, :]
                done.append(summed / pltpu.roll(summed, HEAD_DIM, 1))
            for pair in range(HEADS // 2):
                moved = pltpu.roll(done[2 * pair], HEAD_DIM, 1)
                att[:, pair * TOK : (pair + 1) * TOK] = jnp.where(lane < HEAD_DIM, moved, done[2 * pair + 1]).astype(BF16)
            for step in (2, 1, 3):
                other = (tp + step) % NT
                remote(
                    att.at[pl.ds(pl.multiple_of(other * ROWS, ROWS), ROWS)], planes.at[tp], asend, arecv.at[tp], sp, other
                ).start()

        @pl.when(c == 0)
        def _():
            pass_down()

        load.wait()
        in_copies["res"].wait()
        in_copies["gain"].wait()
        depth = HEADS * HEAD_DIM

        def part_of(rows, group):
            weights = proj[pl.ds(pl.multiple_of(group * depth, depth), depth), :]
            return jnp.dot(rows, weights, preferred_element_type=F32)

        total = part_of(att[pl.ds(pl.multiple_of(tp * ROWS, ROWS), ROWS), :], tp)
        for step in (1, 3, 2):
            other = (tp + step) % NT
            remote(planes.at[other], planes.at[other], asend, arecv.at[other], sp, other).wait_recv()
            total = total + part_of(planes[other], other)
        with jax.named_scope("p_norm"):
            stream = (res_ref[...].astype(F32) + total).astype(BF16)
            kept[...] = stream
            stream = stream.astype(F32)
            normed = stream * lax.rsqrt(jnp.mean(stream * stream, axis=1, keepdims=True) + norm_eps)
            normed = (normed * gain_ref[...]).astype(BF16)
            for piece in range(PIECES):
                stacked[piece * ROWS : (piece + 1) * ROWS, :] = normed[:, piece * WIDE : (piece + 1) * WIDE]

    def dispatch(g):
        plane = (z - ORDER[g] + NZ) % NZ
        rows = pl.ds(pl.multiple_of(plane * TOK, TOK), TOK)
        picked = jnp.dot(chosen[rows, :], stacked[...], preferred_element_type=F32).astype(BF16)
        sent[pl.ds(pl.multiple_of(plane * PLANE, PLANE), PLANE)] = picked.reshape(PLANE, 16, WIDE)

        def one_row(k, carry, plane=plane):
            target = plane * PLANE + (x * NC + c + k) % PLANE
            remote(sent.at[target], came.at[tp, sp], dsend, drecv.at[z], target, tp).start()
            return carry

        if ORDER[g] == 0:
            for step in range(1, PLANE):
                target = plane * PLANE + (x * NC + c + step) % PLANE
                remote(sent.at[target], came.at[tp, sp], dsend, drecv.at[z], target, tp).start()
            pltpu.make_async_copy(sent.at[sp], came.at[tp, sp], drecv.at[z]).start()
        else:
            lax.fori_loop(0, PLANE, one_row, 0)

    def group(ref, source, plane, half=None):
        if half is None:
            return ref.at[source, pl.ds(pl.multiple_of(plane * PLANE, PLANE), PLANE)]
        return ref.at[source, pl.ds(pl.multiple_of(plane * PLANE + half * (PLANE // 2), PLANE // 2), PLANE // 2)]

    def share(g):
        plane = plane_at(g)
        ref = group(came, tp, plane)
        remote(ref, ref, dsend, drecv.at[plane], sp, right).wait_recv()
        remote(ref, ref, ysend, yl.at[g], sp, right).start()
        remote(ref, ref, ysend, yr.at[g], sp, left).start()

    def relay(g):
        plane = plane_at(g)
        ref = group(came, left, plane)
        remote(ref, ref, ysend, yl.at[g], sp, right).wait_recv()
        ref = group(came, left, plane, 0)
        remote(ref, ref, ysend, ya.at[g], sp, right).start()
        ref = group(came, right, plane)
        remote(ref, ref, ysend, yr.at[g], sp, left).wait_recv()
        ref = group(came, right, plane, 1)
        remote(ref, ref, ysend, yb.at[g], sp, left).start()

    def gathered(g):
        plane = plane_at(g)
        ref = group(came, far, plane, 0)
        remote(ref, ref, ysend, ya.at[g], sp, right).wait_recv()
        ref = group(came, far, plane, 1)
        remote(ref, ref, ysend, yb.at[g], sp, right).wait_recv()

    def compute(chunk):
        for k in range(2):
            plane = plane_at(PAIRS[chunk][k])
            for source in range(NT):
                rows = came[source, pl.ds(pl.multiple_of(plane * PLANE, PLANE), PLANE)].reshape(TOK, WIDE)
                ordered = jnp.dot(choose[0], rows, preferred_element_type=F32).astype(BF16)
                q = (k * NT + source) * 16
                for piece in range(PIECES):
                    xrows[q : q + 16, piece * WIDE : (piece + 1) * WIDE] = ordered[piece * 16 : piece * 16 + 16, :]
        rows = xrows[...]
        gate = jnp.dot(rows, w_gate[...], preferred_element_type=F32)
        upper = jnp.dot(rows, w_up[...], preferred_element_type=F32)
        hidden[...] = (gate / (1.0 + jnp.exp(-gate)) * upper).astype(BF16)

    def multiply(chunk):
        part = jnp.dot(hidden[...], w_down[tp], preferred_element_type=F32).astype(BF16)
        for k in range(2):
            for source in range(NT):
                q = (k * NT + source) * 16
                pieces[PAIRS[chunk][k], source] = part[q : q + 16, :]

    def send_hidden(chunk):
        for k in range(2):
            g = PAIRS[chunk][k]
            for source in range(NT):
                q = (k * NT + source) * 16
                hid_out[g, source] = hidden[q : q + 16, :]
            hid_in[g, tp] = hid_out[g, tp]
            for other in (right, left, far):
                remote(hid_out.at[g, other], hid_in.at[g, tp], hsend, hrecv.at[g], sp, other).start()

    def finish(chunk):
        for k in range(2):
            g = PAIRS[chunk][k]
            some = hid_in.at[g, pl.ds(0, NT - 1)]
            remote(some, some, hsend, hrecv.at[g], sp, right).wait_recv()
        total = jnp.zeros((32, D), F32)
        for source in range(NT):
            rows = jnp.concatenate([hid_in[g, source] for g in PAIRS[chunk]], axis=0)
            total = total + jnp.dot(rows, w_down[source], preferred_element_type=F32)
        total = total.astype(BF16)
        for k in range(2):
            hand_back(PAIRS[chunk][k], total[16 * k : 16 * k + 16, :])

    half = D // 2

    def first_halves(g):
        remote(pieces.at[g, far, :, pl.ds(0, half)], half_l.at[g], rsend, ra.at[g], sp, right).start()
        remote(pieces.at[g, far, :, pl.ds(half, half)], half_r.at[g], rsend, rb.at[g], sp, left).start()

    def add_half(g):
        remote(half_l.at[g], half_l.at[g], rsend, ra.at[g], sp, right).wait_recv()
        mine = pieces[g, right]
        to_r[g, :, 0:half] = (mine[:, 0:half].astype(F32) + half_l[g].astype(F32)).astype(BF16)
        to_r[g, :, half:] = mine[:, half:]
        remote(to_r.at[g], full_l.at[g], rsend, rl.at[g], sp, right).start()
        remote(half_r.at[g], half_r.at[g], rsend, rb.at[g], sp, right).wait_recv()
        mine = pieces[g, left]
        to_l[g, :, half:] = (mine[:, half:].astype(F32) + half_r[g].astype(F32)).astype(BF16)
        to_l[g, :, 0:half] = mine[:, 0:half]
        remote(to_l.at[g], full_r.at[g], rsend, rr.at[g], sp, left).start()

    def give_back(g):
        plane = plane_at(g)
        remote(full_l.at[g], full_l.at[g], rsend, rl.at[g], sp, right).wait_recv()
        remote(full_r.at[g], full_r.at[g], rsend, rr.at[g], sp, right).wait_recv()
        total = pieces[g, tp].astype(F32) + full_l[g].astype(F32) + full_r[g].astype(F32)
        hand_back(g, total.astype(BF16))

    def hand_back(g, total):
        plane = plane_at(g)
        stacked = jnp.concatenate([total[:, k * WIDE : (k + 1) * WIDE] for k in range(PIECES)], axis=0)
        mixed = jnp.dot(choose[1], stacked, preferred_element_type=F32).astype(BF16)
        back[pl.ds(pl.multiple_of(g * PLANE, PLANE), PLANE)] = mixed.reshape(PLANE, 16, WIDE)

        def one_row(k, carry):
            k = (x * NC + c + k) % PLANE
            target = plane * PLANE + k
            remote(back.at[g * PLANE + k], final.at[sp], fsend, frecv.at[z], target, tp).start()
            return carry

        if ORDER[g] == 0:
            own = x * NC + c
            for step in range(1, PLANE):
                k = (own + step) % PLANE
                remote(
                    back.at[g * PLANE + k], final.at[sp], fsend, frecv.at[z], plane * PLANE + k, tp
                ).start()
            pltpu.make_async_copy(back.at[g * PLANE + own], final.at[sp], frecv.at[z]).start()
        else:
            lax.fori_loop(0, PLANE, one_row, 0)

    chunks = NZ // 2
    def first_return(chunk):
        @pl.when(c == 1)
        def _():
            for g in PAIRS[chunk]:
                with jax.named_scope(f"add_half{g}"):
                    add_half(g)

    def last_return(chunk):
        @pl.when(c == 1)
        def _():
            for g in PAIRS[chunk]:
                with jax.named_scope(f"back{g}"):
                    give_back(g)

    def from_hidden(chunk):
        @pl.when(c == 0)
        def _():
            if chunk == 0:
                with jax.named_scope("all_down"):
                    all_down()
            with jax.named_scope(f"finish{chunk}"):
                finish(chunk)

    def expert(chunk):
        for g in PAIRS[chunk]:
            with jax.named_scope(f"gathered{g}"):
                gathered(g)
        with jax.named_scope(f"compute{chunk}"):
            compute(chunk)

        @pl.when(c == 0)
        def _():
            send_hidden(chunk)

        @pl.when(c == 1)
        def _():
            with jax.named_scope(f"multiply{chunk}"):
                multiply(chunk)
            for g in PAIRS[chunk]:
                first_halves(g)

    D_, S, R, E, H, A, B = dispatch, share, relay, expert, from_hidden, first_return, last_return
    for step, number in (
        (D_, 0), (D_, 1), (D_, 2), (D_, 3), (D_, 4), (S, 0), (D_, 5), (D_, 6), (D_, 7), (S, 1), (R, 0), (S, 2), (S, 3),
        (R, 1), (R, 2), (S, 4), (S, 5), (S, 6), (S, 7), (R, 3), (E, 0), (R, 4), (R, 5), (R, 6), (R, 7), (A, 0), (E, 1),
        (H, 0), (E, 2), (B, 0), (A, 1), (E, 3), (H, 1), (A, 2), (B, 1), (H, 2), (A, 3), (B, 2), (H, 3), (B, 3),
    ):
        with jax.named_scope(f"{step.__name__}{number}"):
            step(number)

    some = sent.at[pl.ds(0, experts - 1)]
    remote(some, some, dsend, drecv.at[0], sp, right).wait_send()
    some = came.at[pl.ds(0, 3)]
    remote(some, some, ysend, yl.at[0], sp, right).wait_send()

    @pl.when(c == 0)
    def _():
        some = w_down.at[pl.ds(0, 3)]
        remote(some, some, gsend, gl.at[0], sp, right).wait_send()
        some = hid_in.at[pl.ds(0, 6)]
        remote(some, some, hsend, hrecv.at[0], sp, right).wait_send()

    @pl.when(c == 1)
    def _():
        some = pieces.at[pl.ds(0, 6)]
        remote(some, some, rsend, ra.at[0], sp, right).wait_send()


    count = 5 + 15 + 20
    remote(kvg.at[pl.ds(0, count)], kvg.at[pl.ds(0, count)], send, recv.at[0], sp, (tp + 1) % NT).wait_send()
    remote(planes.at[pl.ds(0, 3)], planes.at[pl.ds(0, 3)], asend, arecv.at[0], sp, (tp + 1) % NT).wait_send()

    columns = turn[...].T[0:ROWS, :]
    for first, g in enumerate(g for pair in PAIRS for g in pair):
        plane = (z - ORDER[g] + NZ) % NZ
        ref = final.at[pl.ds(pl.multiple_of(plane * PLANE, PLANE), PLANE)]
        with jax.named_scope(f"take{g}"):
            remote(ref, ref, fsend, frecv.at[plane], sp, right).wait_recv()
        rows = final[pl.ds(pl.multiple_of(plane * PLANE, PLANE), PLANE)].reshape(TOK, WIDE)
        part = jnp.dot(pick[plane], rows, preferred_element_type=F32)
        taken[...] = part if first == 0 else taken[...] + part
    weight0, weight1 = columns[:, 2:3], columns[:, 3:4]
    for piece in range(PIECES):
        lanes = slice(piece * WIDE, (piece + 1) * WIDE)
        one = taken[piece * ROWS : (piece + 1) * ROWS, :]
        two = taken[(PIECES + piece) * ROWS : (PIECES + piece + 1) * ROWS, :]
        out_ref[:, lanes] = (kept[:, lanes].astype(F32) + (weight0 * one + weight1 * two)).astype(BF16)

    some = final.at[pl.ds(0, experts - 1)]
    remote(some, some, fsend, frecv.at[0], sp, right).wait_send()


def local(
    queries, keys, values, cum_gate, doc_ids, residual, out_proj, norm_gain, route_ids, route_weights,
    expert_gate, expert_up, expert_down,
):
    anywhere = pl.BlockSpec(memory_space=pl.ANY)
    dma, experts = pltpu.SemaphoreType.DMA, NZ * PLANE
    wide_heads = HEADS * HEAD_DIM
    return pl.pallas_call(
        layer_kernel,
        out_shape=pltpu.VMEM((ROWS, D), BF16),
        in_specs=[anywhere] * 13,
        out_specs=pl.BlockSpec(memory_space=pltpu.VMEM),
        scratch_shapes=[
            pltpu.VMEM((TOK, wide_heads), BF16),
            pltpu.VMEM((HEADS, TOK), F32),
            pltpu.VMEM((1, TOK), jnp.int32),
            pltpu.VMEM((ROWS, D), BF16),
            pltpu.VMEM((1, D), F32),
            pltpu.VMEM((2, ROWS), jnp.int32),
            pltpu.VMEM((2, ROWS), F32),
            pltpu.VMEM((experts, BLK, TOK), BF16),
            pltpu.VMEM((8, TOK), F32),
            pltpu.VMEM((HEADS * TOK, TOK), BF16),
            pltpu.VMEM((8, (PLANE + 1) * TOK), F32),
            pltpu.VMEM((HEADS * TOK, TOK), F32),
            pltpu.VMEM((HEADS * TOK, TOK), F32),
            pltpu.VMEM((HEADS * TOK, (PLANE + 1) * TOK), BF16),
            pltpu.VMEM(((PLANE + 1) * TOK, TOK), BF16),
            pltpu.VMEM((TOK, wide_heads), BF16),
            pltpu.VMEM((NT, ROWS, wide_heads), BF16),
            pltpu.VMEM((NT * wide_heads, D), BF16),
            pltpu.VMEM((ROWS, D), BF16),
            pltpu.VMEM((PIECES * ROWS, WIDE), BF16),
            pltpu.VMEM((TOK, TOK), F32),
            pltpu.VMEM((experts * 16, WIDE), BF16),
            pltpu.VMEM((2, TOK, TOK), BF16),
            pltpu.VMEM((experts, 16, WIDE), BF16),
            pltpu.VMEM((NT, experts, 16, WIDE), BF16),
            pltpu.VMEM((NZ, 2 * PIECES * ROWS, TOK), BF16),
            pltpu.VMEM((TOK, D), BF16),
            pltpu.VMEM((D, WIDE), BF16),
            pltpu.VMEM((D, WIDE), BF16),
            pltpu.VMEM((NT, WIDE, D), BF16),
            pltpu.VMEM((TOK, WIDE), BF16),
            pltpu.VMEM((NZ, NT, 16, WIDE), BF16),
            pltpu.VMEM((NZ, NT, 16, WIDE), BF16),
            pltpu.VMEM((NZ, NT, 16, D), BF16),
            pltpu.VMEM((NZ, 16, D // 2), BF16),
            pltpu.VMEM((NZ, 16, D // 2), BF16),
            pltpu.VMEM((NZ, 16, D), BF16),
            pltpu.VMEM((NZ, 16, D), BF16),
            pltpu.VMEM((NZ, 16, D), BF16),
            pltpu.VMEM((NZ, 16, D), BF16),
            pltpu.VMEM((experts, 16, WIDE), BF16),
            pltpu.VMEM((experts, 16, WIDE), BF16),
            pltpu.VMEM((2 * PIECES * ROWS, WIDE), F32),
            dma((9,)), dma((experts,)), dma, dma((NT,)), dma, dma,
            dma((3,)), dma, dma((NZ,)), dma, dma((NZ,)), dma((NZ,)), dma((NZ,)), dma((NZ,)),
            dma, dma((NZ,)), dma((NZ,)), dma((NZ,)), dma((NZ,)), dma, dma((NZ,)),
            dma, dma((3,)), dma((3,)), dma, dma((NZ,)),
        ],
        compiler_params=pltpu.CompilerParams(
            collective_id=0, has_side_effects=True, vmem_limit_bytes=60 << 20
        ),
        name="layer",
    )(
        queries, keys.T, values.T, cum_gate.T, doc_ids[None], residual, norm_gain[None], out_proj,
        route_ids.T, route_weights.T, expert_gate, expert_up, expert_down,
    )


def solution(mesh):
    in_specs = (
        P("sp", "tp"),
        P("sp", "tp"),
        P("sp", "tp"),
        P("sp", "tp"),
        P("sp"),
        P(("sp", "tp"), None),
        P(),
        P(),
        P(("sp", "tp"), None),
        P(("sp", "tp"), None),
        P("sp", None, "tp"),
        P("sp", None, "tp"),
        P("sp", "tp", None),
    )
    out_specs = P(("sp", "tp"), None)
    return jax.shard_map(local, mesh=mesh, in_specs=in_specs, out_specs=out_specs, check_vma=False)
```
